512 devices in a mesh: grp: 2 (over y), kv: 16 (over z), tp: 16 (over x, core).
Axes of the slice: x: 8, y: 2, z: 16, core: 2. Of those that a mesh axis runs over, the one named last changes fastest.
The devices are a block of a 8x16x16 slice.
Arguments:
- stream_in: bfloat16 [384, 4096], P(('grp', 'tp'), 'kv'), parts along dimension 0, may hold values from -40 to 40
- positions: int32 [384], P(('grp', 'kv')), parts along dimension 0, may hold values from 1024 to 32767
- ret_state: float32 [384, 16, 128, 128], P(('grp', 'kv'), 'tp'), parts along dimension 0, may hold values from -0.6 to 0.6
- first_gain: float32 [4096], P('kv'), may hold values from 0.1 to 1.9
- first_gate: bfloat16 [4096, 11008], P('kv', 'tp'), may hold values from -0.09375 to 0.09375
- first_up: bfloat16 [4096, 11008], P('kv', 'tp'), may hold values from -0.09375 to 0.09375
- first_down: bfloat16 [11008, 4096], P('tp', 'kv'), may hold values from -0.1875 to 0.1875
- mix_gain: float32 [4096], P('kv'), may hold values from 0.1 to 1.9
- w_query: bfloat16 [4096, 2048], P('kv', 'tp'), may hold values from -0.09375 to 0.09375
- w_key: bfloat16 [4096, 2048], P('kv', 'tp'), may hold values from -0.09375 to 0.09375
- w_value: bfloat16 [4096, 2048], P('kv', 'tp'), may hold values from -0.09375 to 0.09375
- w_outgate: bfloat16 [4096, 2048], P('kv', 'tp'), may hold values from -0.09375 to 0.09375
- w_out: bfloat16 [2048, 4096], P('tp', 'kv'), may hold values from -0.21875 to 0.21875
- head_gain: float32 [2048], P('tp'), may hold values from 0.1 to 1.9
- second_gain: float32 [4096], P('kv'), may hold values from 0.1 to 1.9
- second_gate: bfloat16 [4096, 11008], P('kv', 'tp'), may hold values from -0.09375 to 0.09375
- second_up: bfloat16 [4096, 11008], P('kv', 'tp'), may hold values from -0.09375 to 0.09375
- second_down: bfloat16 [11008, 4096], P('tp', 'kv'), may hold values from -0.1875 to 0.1875
Outputs:
- stream_out: bfloat16 [384, 4096], P(('grp', 'tp'), 'kv'), parts along dimension 0
- new_state: float32 [384, 16, 128, 128], P(('grp', 'kv'), 'tp'), parts along dimension 0
The draws below stay inside these ranges and needn't reach their ends.
There are 2 independent parts, one for each index of `grp`. The reference program is written for one: setup_inputs(seed, part) draws one part's arguments, and reference() takes and returns one part's arrays. A program takes and returns all parts, laid end to end along the dimension named above; an argument that names none is the same for every part. Nothing has to cross between parts.
All inputs are finite; a program needn't handle non-finite values.
Results may differ from the reference program's by a relative error of at most 0.03.
Values may be sent and summed in bfloat16 or wider, within the bound.
No kernel may reach another device: no remote copies, remote signals or barrier semaphores. Data moves between devices by JAX's collectives and lax.ppermute only.
A program may use at most 64 MiB of HBM per device.

```python
import jax
import jax.numpy as jnp
from jax import lax

D = 4096
FF = 11008
HEADS = 16
HEAD_DIM = 128
BATCH = 192
RET_WIDTH = 2048


def draw_stream_in(key, part):
    base_key, column_key, row_key = jax.random.split(jax.random.fold_in(key, 17), 3)
    columns = jnp.arange(D, dtype=jnp.float32) / D
    base = jax.random.truncated_normal(base_key, -4.0, 4.0, (BATCH, D), jnp.float32)
    column_scale = jnp.exp(0.5 * jnp.log(10.0) * (columns + jax.random.uniform(column_key, (D,), jnp.float32)))
    row_scale = jnp.exp(jax.random.uniform(row_key, (BATCH, 1), jnp.float32, 0.0, jnp.log(3.0)))
    return (0.3 * base * column_scale[None, :] * row_scale).astype(jnp.bfloat16)


def place_ends(result, stream_key, least, largest):
    place = [jax.random.randint(jax.random.fold_in(stream_key, axis), (), 0, length) for axis, length in enumerate(result.shape)]
    widest = result.shape.index(max(result.shape))
    neighbour = place[:widest] + [(place[widest] + 1) % result.shape[widest]] + place[widest + 1:]
    return result.at[tuple(place)].set(least).at[tuple(neighbour)].set(largest)


def block_levels(key, dims, cuts, low, high):
    loudness, own = 1.0, jax.random.fold_in(key, 6)
    for position, shards_of in cuts:
        draws = jnp.exp(jax.random.uniform(jax.random.fold_in(own, position), (shards_of,), jnp.float32, low / len(cuts), high / len(cuts)))
        loudness = loudness * jnp.repeat(draws, dims[position] // shards_of).reshape([-1 if axis == position else 1 for axis in range(len(dims))])
    return loudness


def bell_draw(rng, dims, width, limit, cuts=(), kind=jnp.bfloat16):
    loudness = block_levels(rng, dims, cuts, -0.22, 0.18) if cuts else 1.0
    values = jax.random.normal(rng, dims, jnp.float32) * width * loudness
    return jnp.minimum(jnp.maximum(values, -limit), limit).astype(kind)


def setup_inputs(seed: int = 0, part: int = 0) -> dict:
    keys = jax.random.split(jax.random.key(seed), 19)
    part_splits = jax.random.split(jax.random.fold_in(keys[18], part), 19)
    stream_in = draw_stream_in(jax.random.fold_in(jax.random.fold_in(keys[18], part), 71), part)
    positions = place_ends(jax.random.randint(part_splits[1], (BATCH,), 1024, 32768), jax.random.fold_in(part_splits[1], 1), 1024, 32767).astype(jnp.int32)
    ret_state = bell_draw(part_splits[2], (BATCH, HEADS, HEAD_DIM, HEAD_DIM), 0.1, 0.6, ((0, 16), (1, 16)), jnp.float32)
    first_gain = jnp.clip(1.0 + 0.18 * jax.random.normal(keys[3], (D,), jnp.float32), 0.1, 1.9)
    first_gate = bell_draw(keys[4], (D, FF), D ** -0.5, 0.09375, ((0, 16), (1, 16)))
    first_up = bell_draw(keys[5], (D, FF), D ** -0.5, 0.09375, ((0, 16), (1, 16)))
    first_down = bell_draw(keys[6], (FF, D), (FF // 12) ** -0.5, 0.1875, ((0, 16), (1, 16)))
    mix_gain = jnp.clip(1.0 + 0.18 * jax.random.normal(keys[7], (D,), jnp.float32), 0.1, 1.9)
    w_query = bell_draw(keys[8], (D, RET_WIDTH), D ** -0.5, 0.09375, ((0, 16), (1, 16)))
    w_key = bell_draw(keys[9], (D, RET_WIDTH), D ** -0.5, 0.09375, ((0, 16), (1, 16)))
    w_value = bell_draw(keys[10], (D, RET_WIDTH), D ** -0.5, 0.09375, ((0, 16), (1, 16)))
    w_outgate = bell_draw(keys[11], (D, RET_WIDTH), D ** -0.5, 0.09375, ((0, 16), (1, 16)))
    w_out = bell_draw(keys[12], (RET_WIDTH, D), (RET_WIDTH // 3) ** -0.5, 0.21875, ((0, 16), (1, 16)))
    head_gain = jnp.clip(1.0 + 0.18 * jax.random.normal(keys[13], (RET_WIDTH,), jnp.float32), 0.1, 1.9)
    second_gain = jnp.clip(1.0 + 0.18 * jax.random.normal(keys[14], (D,), jnp.float32), 0.1, 1.9)
    second_gate = bell_draw(keys[15], (D, FF), D ** -0.5, 0.09375, ((0, 16), (1, 16)))
    second_up = bell_draw(keys[16], (D, FF), D ** -0.5, 0.09375, ((0, 16), (1, 16)))
    second_down = bell_draw(keys[17], (FF, D), (FF // 12) ** -0.5, 0.1875, ((0, 16), (1, 16)))
    return {"stream_in": stream_in, "positions": positions, "ret_state": ret_state, "first_gain": first_gain, "first_gate": first_gate, "first_up": first_up, "first_down": first_down, "mix_gain": mix_gain, "w_query": w_query, "w_key": w_key, "w_value": w_value, "w_outgate": w_outgate, "w_out": w_out, "head_gain": head_gain, "second_gain": second_gain, "second_gate": second_gate, "second_up": second_up, "second_down": second_down}


EPS_NORM = 1e-06
EPS_GROUP = 1e-05

def prepare(stream, norm_gain):
    widened = stream.astype(jnp.float32)
    squares = lax.optimization_barrier(jnp.sum(widened * widened, axis=1))
    scaled = (widened * norm_gain.astype(jnp.float32)).astype(jnp.bfloat16)
    factor = lax.rsqrt(squares / D + EPS_NORM)[:, None]
    return (factor, scaled)

def feed_forward(stream, norm_gain, w_gate, w_up, w_down):
    factor, scaled = prepare(stream, norm_gain)
    gate_pre = factor * jnp.dot(scaled, w_gate, preferred_element_type=jnp.float32)
    up_pre = factor * jnp.dot(scaled, w_up, preferred_element_type=jnp.float32)
    hidden = (jax.nn.silu(gate_pre) * up_pre).astype(jnp.bfloat16)
    return (stream.astype(jnp.float32) + 0.5 * jnp.dot(hidden, w_down, preferred_element_type=jnp.float32)).astype(jnp.bfloat16)

def rotate(values_in, cosine, sine_part):
    half_dim = values_in.shape[-1] // 2
    lower_half = values_in[..., :half_dim]
    upper_half = values_in[..., half_dim:]
    return jnp.concatenate([lower_half * cosine - upper_half * sine_part, lower_half * sine_part + upper_half * cosine], axis=-1)

def reference(stream_in, positions, ret_state, first_gain, first_gate, first_up, first_down, mix_gain, w_query, w_key, w_value, w_outgate, w_out, head_gain, second_gain, second_gate, second_up, second_down):
    stream = feed_forward(stream_in, first_gain, first_gate, first_up, first_down)
    factor, scaled = prepare(stream, mix_gain)
    shape_heads = (BATCH, HEADS, HEAD_DIM)
    queries = (factor * jnp.dot(scaled, w_query, preferred_element_type=jnp.float32)).reshape(shape_heads)
    key_vec = (factor * jnp.dot(scaled, w_key, preferred_element_type=jnp.float32)).reshape(shape_heads)
    values_new = (factor * jnp.dot(scaled, w_value, preferred_element_type=jnp.float32)).reshape(shape_heads)
    gate_pre = (factor * jnp.dot(scaled, w_outgate, preferred_element_type=jnp.float32)).reshape(shape_heads)
    half_dim = HEAD_DIM // 2
    inverse = 10000.0 ** (-jnp.arange(half_dim, dtype=jnp.float32) / half_dim)
    angles = positions.astype(jnp.float32)[:, None] * inverse[None, :]
    cosine = jnp.cos(angles)[:, None, :]
    sine_part = jnp.sin(angles)[:, None, :]
    queries = rotate(queries, cosine, sine_part)
    key_vec = rotate(key_vec, cosine, sine_part) * HEAD_DIM ** (-0.5)
    head_ids = jnp.arange(HEADS).astype(jnp.float32)
    decays = jnp.exp(jnp.log1p(-2.0 ** (-5.0 - head_ids)))
    carried = jnp.einsum('shd,shde->she', queries, ret_state, precision=lax.Precision.HIGHEST)
    within = lax.optimization_barrier(jnp.sum(queries * key_vec, axis=-1, keepdims=True))
    mixture = decays[None, :, None] * carried + within * values_new
    new_state = decays[None, :, None, None] * ret_state + key_vec[..., :, None] * values_new[..., None, :]
    average = lax.optimization_barrier(jnp.mean(mixture, axis=-1, keepdims=True))
    centered = mixture - average
    variance = lax.optimization_barrier(jnp.mean(centered * centered, axis=-1, keepdims=True))
    normed = centered * lax.rsqrt(variance + EPS_GROUP) * head_gain.astype(jnp.float32).reshape(HEADS, HEAD_DIM)
    ret_out = (jax.nn.silu(gate_pre) * normed).astype(jnp.bfloat16).reshape(BATCH, RET_WIDTH)
    stream = (stream.astype(jnp.float32) + jnp.dot(ret_out, w_out, preferred_element_type=jnp.float32)).astype(jnp.bfloat16)
    stream = feed_forward(stream, second_gain, second_gate, second_up, second_down)
    return (stream, new_state)
```

```python
import jax
import jax.numpy as jnp
from jax import lax
from jax.sharding import PartitionSpec as P

EPS_NORM = 1e-06
EPS_GROUP = 1e-05
CHAINS = ((0, 8), (8, 4))


def exchange(x, axis):
    return lax.all_to_all(x, axis, split_axis=0, concat_axis=0, tiled=True)


def summed(x, axis):
    return exchange(x, axis).astype(jnp.float32).sum(axis=0)


def spread(x, axis):
    return exchange(jnp.broadcast_to(x[None], (lax.axis_size(axis), *x.shape)), axis)


def prepare(stream, norm_gain):
    widened = stream.astype(jnp.float32)
    squares = jnp.sum(widened * widened, axis=1, keepdims=True).astype(jnp.bfloat16)
    return squares, (widened * norm_gain).astype(jnp.bfloat16)


def dot(a, b):
    return jnp.dot(a, b, preferred_element_type=jnp.float32)


def feed_forward(stream, norm_gain, w_gate, w_up, w_down):
    members = lax.axis_size("kv")
    rows, width = stream.shape[0], w_gate.shape[1]
    tall = rows // members
    cuts = 1
    while (tall * cuts) % 8:
        cuts *= 2
    tall, part = tall * cuts, width // cuts
    features = lax.axis_size("kv") * stream.shape[1]
    squares, scaled = prepare(stream, norm_gain)
    pieces = []
    for c in range(cuts):
        gate = dot(scaled, w_gate[:, c * part : (c + 1) * part]).astype(jnp.bfloat16)
        up = dot(scaled, w_up[:, c * part : (c + 1) * part]).astype(jnp.bfloat16)
        piece = jnp.concatenate([gate, up, squares], axis=1)
        pieces.append(piece.reshape(members // cuts, tall, 2 * part + 1))
    sent = pieces[0] if cuts == 1 else jnp.stack(pieces, axis=1).reshape(members, tall, 2 * part + 1)
    total = summed(sent, "kv")
    factor = lax.rsqrt(total[:, 2 * part :] / features + EPS_NORM)
    hidden = (jax.nn.silu(factor * total[:, :part]) * (factor * total[:, part : 2 * part])).astype(jnp.bfloat16)
    everyone = spread(hidden, "kv").reshape(members // cuts, cuts, tall, part)
    back = 0.0
    for c in range(cuts):
        back += dot(everyone[:, c].reshape(rows, part), w_down[c * part : (c + 1) * part])
    return back


def advance(own, back, branch):
    members = lax.axis_size("tp")
    share = summed(back.astype(jnp.bfloat16).reshape(members, -1, back.shape[1]), "tp")
    return (own.astype(jnp.float32) + branch * share).astype(jnp.bfloat16)


def widen(own):
    gathered = spread(own, "tp")
    return gathered.reshape(-1, own.shape[1])


def rotate(values_in, cosine, sine):
    half = values_in.shape[-1] // 2
    low, high = values_in[..., :half], values_in[..., half:]
    return jnp.concatenate([low * cosine - high * sine, low * sine + high * cosine], axis=-1)


def retention(stream, norm_gain, w_heads, head_gain, state, positions):
    members = lax.axis_size("kv")
    features = members * stream.shape[1]
    squares, scaled = prepare(stream, norm_gain)
    parts = [dot(scaled, w).astype(jnp.bfloat16) for w in w_heads]
    sent = jnp.concatenate([*parts, squares], axis=1).reshape(members, -1, 4 * parts[0].shape[1] + 1)
    total = summed(sent, "kv")
    count, heads, width, _ = state.shape
    factor = lax.rsqrt(total[:, 4 * heads * width :] / features + EPS_NORM)
    shape = (count, heads, width)
    q, k, v, o = ((factor * total[:, i * heads * width : (i + 1) * heads * width]).reshape(shape) for i in range(4))
    half = width // 2
    inverse = 10000.0 ** (-jnp.arange(half, dtype=jnp.float32) / half)
    angles = positions.astype(jnp.float32)[:, None] * inverse[None, :]
    cosine, sine = jnp.cos(angles)[:, None, :], jnp.sin(angles)[:, None, :]
    q = rotate(q, cosine, sine)
    k = rotate(k, cosine, sine) * width ** (-0.5)
    head_ids = (lax.axis_index("tp") * heads + jnp.arange(heads)).astype(jnp.float32)
    decays = jnp.exp(jnp.log1p(-(2.0 ** (-5.0 - head_ids))))
    carried = jnp.einsum("shd,shde->she", q, state, precision=lax.Precision.HIGHEST)
    within = jnp.sum(q * k, axis=-1, keepdims=True)
    mixture = decays[None, :, None] * carried + within * v
    centered = mixture - jnp.mean(mixture, axis=-1, keepdims=True)
    variance = jnp.mean(centered * centered, axis=-1, keepdims=True)
    normed = centered * lax.rsqrt(variance + EPS_GROUP) * head_gain.reshape(heads, width)
    ret_out = (jax.nn.silu(o) * normed).astype(jnp.bfloat16).reshape(count, heads * width)
    new_state = decays[None, :, None, None] * state + k[..., :, None] * v[..., None, :]
    return spread(ret_out, "kv").reshape(stream.shape[0], heads * width), new_state


def per_device(
    stream_in,
    positions,
    ret_state,
    first_gain,
    first_gate,
    first_up,
    first_down,
    mix_gain,
    w_query,
    w_key,
    w_value,
    w_outgate,
    w_out,
    head_gain,
    second_gain,
    second_gate,
    second_up,
    second_down,
):
    outs, states = [], []
    for start, count in CHAINS:
        own = stream_in[start : start + count]
        stream = widen(own)
        back = feed_forward(stream, first_gain, first_gate, first_up, first_down)
        own = advance(own, back, 0.5)
        stream = widen(own)
        ret_out, state = retention(
            stream,
            mix_gain,
            (w_query, w_key, w_value, w_outgate),
            head_gain,
            ret_state[start : start + count],
            positions[start : start + count],
        )
        own = advance(own, dot(ret_out, w_out), 1.0)
        stream = widen(own)
        back = feed_forward(stream, second_gain, second_gate, second_up, second_down)
        outs.append(advance(own, back, 0.5))
        states.append(state)
    return jnp.concatenate(outs, axis=0), jnp.concatenate(states, axis=0)


def solution(mesh):
    in_specs = (
        P(("grp", "tp"), "kv"),
        P(("grp", "kv")),
        P(("grp", "kv"), "tp", None, None),
        P("kv"),
        P("kv", "tp"),
        P("kv", "tp"),
        P("tp", "kv"),
        P("kv"),
        P("kv", "tp"),
        P("kv", "tp"),
        P("kv", "tp"),
        P("kv", "tp"),
        P("tp", "kv"),
        P("tp"),
        P("kv"),
        P("kv", "tp"),
        P("kv", "tp"),
        P("tp", "kv"),
    )
    out_specs = (P(("grp", "tp"), "kv"), P(("grp", "kv"), "tp", None, None))
    return jax.shard_map(
        per_device, mesh=mesh, in_specs=in_specs, out_specs=out_specs, check_vma=False
    )
```

```python
import jax
import jax.numpy as jnp
from jax import lax
from jax.sharding import PartitionSpec as P

EPS_NORM = 1e-06
EPS_GROUP = 1e-05
CHAINS = ((0, 12),)


def exchange(x, axis):
    return lax.all_to_all(x, axis, split_axis=0, concat_axis=0, tiled=True)


def summed(x, axis):
    return exchange(x, axis).astype(jnp.float32).sum(axis=0)


def spread(x, axis):
    return exchange(jnp.broadcast_to(x[None], (lax.axis_size(axis), *x.shape)), axis)


def prepare(stream, norm_gain):
    widened = stream.astype(jnp.float32)
    squares = jnp.sum(widened * widened, axis=1, keepdims=True).astype(jnp.bfloat16)
    return squares, (widened * norm_gain).astype(jnp.bfloat16)


def dot(a, b):
    return jnp.dot(a, b, preferred_element_type=jnp.float32)


def feed_forward(stream, norm_gain, w_gate, w_up, w_down):
    members = lax.axis_size("kv")
    rows, width = stream.shape[0], w_gate.shape[1]
    tall = rows // members
    cuts = 1
    while (tall * cuts) % 8:
        cuts *= 2
    tall, part = tall * cuts, width // cuts
    features = lax.axis_size("kv") * stream.shape[1]
    squares, scaled = prepare(stream, norm_gain)
    pieces = []
    for c in range(cuts):
        gate = dot(scaled, w_gate[:, c * part : (c + 1) * part]).astype(jnp.bfloat16)
        up = dot(scaled, w_up[:, c * part : (c + 1) * part]).astype(jnp.bfloat16)
        piece = jnp.concatenate([gate, up, squares], axis=1)
        pieces.append(piece.reshape(members // cuts, tall, 2 * part + 1))
    sent = pieces[0] if cuts == 1 else jnp.stack(pieces, axis=1).reshape(members, tall, 2 * part + 1)
    total = summed(sent, "kv")
    factor = lax.rsqrt(total[:, 2 * part :] / features + EPS_NORM)
    hidden = (jax.nn.silu(factor * total[:, :part]) * (factor * total[:, part : 2 * part])).astype(jnp.bfloat16)
    everyone = spread(hidden, "kv").reshape(members // cuts, cuts, tall, part)
    back = 0.0
    for c in range(cuts):
        back += dot(everyone[:, c].reshape(rows, part), w_down[c * part : (c + 1) * part])
    return back


def advance(own, back, branch):
    members = lax.axis_size("tp")
    share = summed(back.astype(jnp.bfloat16).reshape(members, -1, back.shape[1]), "tp")
    return (own.astype(jnp.float32) + branch * share).astype(jnp.bfloat16)


def widen(own):
    gathered = spread(own, "tp")
    return gathered.reshape(-1, own.shape[1])


def rotate(values_in, cosine, sine):
    half = values_in.shape[-1] // 2
    low, high = values_in[..., :half], values_in[..., half:]
    return jnp.concatenate([low * cosine - high * sine, low * sine + high * cosine], axis=-1)


def retention(stream, norm_gain, w_heads, head_gain, state, positions):
    members = lax.axis_size("kv")
    features = members * stream.shape[1]
    squares, scaled = prepare(stream, norm_gain)
    parts = [dot(scaled, w).astype(jnp.bfloat16) for w in w_heads]
    sent = jnp.concatenate([*parts, squares], axis=1).reshape(members, -1, 4 * parts[0].shape[1] + 1)
    total = summed(sent, "kv")
    count, heads, width, _ = state.shape
    factor = lax.rsqrt(total[:, 4 * heads * width :] / features + EPS_NORM)
    shape = (count, heads, width)
    q, k, v, o = ((factor * total[:, i * heads * width : (i + 1) * heads * width]).reshape(shape) for i in range(4))
    half = width // 2
    inverse = 10000.0 ** (-jnp.arange(half, dtype=jnp.float32) / half)
    angles = positions.astype(jnp.float32)[:, None] * inverse[None, :]
    cosine, sine = jnp.cos(angles)[:, None, :], jnp.sin(angles)[:, None, :]
    q = rotate(q, cosine, sine)
    k = rotate(k, cosine, sine) * width ** (-0.5)
    head_ids = (lax.axis_index("tp") * heads + jnp.arange(heads)).astype(jnp.float32)
    decays = jnp.exp(jnp.log1p(-(2.0 ** (-5.0 - head_ids))))
    carried = jnp.einsum("shd,shde->she", q, state, precision=lax.Precision.HIGHEST)
    within = jnp.sum(q * k, axis=-1, keepdims=True)
    mixture = decays[None, :, None] * carried + within * v
    centered = mixture - jnp.mean(mixture, axis=-1, keepdims=True)
    variance = jnp.mean(centered * centered, axis=-1, keepdims=True)
    normed = centered * lax.rsqrt(variance + EPS_GROUP) * head_gain.reshape(heads, width)
    ret_out = (jax.nn.silu(o) * normed).astype(jnp.bfloat16).reshape(count, heads * width)
    new_state = decays[None, :, None, None] * state + k[..., :, None] * v[..., None, :]
    return spread(ret_out, "kv").reshape(stream.shape[0], heads * width), new_state


def per_device(
    stream_in,
    positions,
    ret_state,
    first_gain,
    first_gate,
    first_up,
    first_down,
    mix_gain,
    w_query,
    w_key,
    w_value,
    w_outgate,
    w_out,
    head_gain,
    second_gain,
    second_gate,
    second_up,
    second_down,
):
    outs, states = [], []
    for start, count in CHAINS:
        own = stream_in[start : start + count]
        stream = widen(own)
        back = feed_forward(stream, first_gain, first_gate, first_up, first_down)
        own = advance(own, back, 0.5)
        stream = widen(own)
        ret_out, state = retention(
            stream,
            mix_gain,
            (w_query, w_key, w_value, w_outgate),
            head_gain,
            ret_state[start : start + count],
            positions[start : start + count],
        )
        own = advance(own, dot(ret_out, w_out), 1.0)
        stream = widen(own)
        back = feed_forward(stream, second_gain, second_gate, second_up, second_down)
        outs.append(advance(own, back, 0.5))
        states.append(state)
    return jnp.concatenate(outs, axis=0), jnp.concatenate(states, axis=0)


def solution(mesh):
    in_specs = (
        P(("grp", "tp"), "kv"),
        P(("grp", "kv")),
        P(("grp", "kv"), "tp", None, None),
        P("kv"),
        P("kv", "tp"),
        P("kv", "tp"),
        P("tp", "kv"),
        P("kv"),
        P("kv", "tp"),
        P("kv", "tp"),
        P("kv", "tp"),
        P("kv", "tp"),
        P("tp", "kv"),
        P("tp"),
        P("kv"),
        P("kv", "tp"),
        P("kv", "tp"),
        P("tp", "kv"),
    )
    out_specs = (P(("grp", "tp"), "kv"), P(("grp", "kv"), "tp", None, None))
    return jax.shard_map(
        per_device, mesh=mesh, in_specs=in_specs, out_specs=out_specs, check_vma=False
    )
```

```python
import functools

import jax
import jax.numpy as jnp
import numpy as np
from jax import lax
from jax.experimental import pallas as pl
from jax.experimental.pallas import tpu as pltpu
from jax.sharding import Mesh
from jax.sharding import PartitionSpec as P

EPS_NORM = 1e-06
EPS_GROUP = 1e-05
KV = ("kvh", "kvp")
BOTH = ("kvp", "tp")
VMEM = pl.BlockSpec(memory_space=pltpu.VMEM)
NT = (((1,), (1,)), ((), ()))


def local_call(kernel, out_shape, *args, scratch=(), flops=0):
    return pl.pallas_call(
        kernel,
        out_shape=out_shape,
        in_specs=[VMEM] * len(args),
        out_specs=jax.tree.map(lambda _: VMEM, out_shape),
        scratch_shapes=scratch,
        cost_estimate=pl.CostEstimate(flops=flops, bytes_accessed=2**20, transcendentals=0),
        compiler_params=pltpu.CompilerParams(vmem_limit_bytes=16 * 2**20),
    )(*args)


def exchange(x, axis):
    return lax.all_to_all(x, axis, split_axis=0, concat_axis=0, tiled=True)


def spread(x, axis):
    return exchange(jnp.broadcast_to(x[None], (lax.axis_size(axis), *x.shape)), axis)


def mine(x, index):
    return lax.dynamic_index_in_dim(x, index, 0, keepdims=False)


def fill_rows(x, y_ref, p):
    if len(y_ref.shape) == 3:
        x[0] = y_ref[p]
        x[1] = y_ref[1 - p]
        return
    _, chunks, tall, wide = y_ref.shape
    across = x.shape[2] // wide
    for n in range(chunks):
        r, c = divmod(n, across)
        place = (slice(r * tall, (r + 1) * tall), slice(c * wide, (c + 1) * wide))
        x[(0, *place)] = y_ref[p, n]
        x[(1, *place)] = y_ref[1 - p, n]


def up_kernel(y_ref, own_ref, got_ref, out_ref, x):
    fill_rows(x, y_ref, lax.axis_index("kvp"))
    groups, tall, lanes = out_ref.shape
    part = own_ref.shape[1]
    half = lanes // 2
    squares = sum(jnp.sum(jnp.square(x[j].astype(jnp.float32)), axis=1, keepdims=True) for j in range(2))
    for i in range(2):
        value = sum(
            lax.dot_general(x[j], w[i], NT, preferred_element_type=jnp.float32)
            for j, w in enumerate((own_ref, got_ref))
        )
        rows = jnp.concatenate([value, jnp.broadcast_to(squares, (value.shape[0], half - part))], axis=1)
        rows = rows.astype(jnp.bfloat16)
        for r in range(groups):
            out_ref[r, :, i * half : (i + 1) * half] = rows[r * tall : (r + 1) * tall]


def down_kernel(h_ref, w_ref, out_ref, h):
    groups, tall, part = h_ref.shape
    cuts = w_ref.shape[0] // part
    value = 0.0
    for c in range(cuts):
        for r in range(groups // cuts):
            h[r * tall : (r + 1) * tall] = h_ref[r * cuts + c]
        value += jnp.dot(h[...], w_ref[c * part : (c + 1) * part], preferred_element_type=jnp.float32)
    value = value.astype(jnp.bfloat16)
    if len(out_ref.shape) == 2:
        out_ref[...] = value
        return
    chunks, high, wide = out_ref.shape
    across = value.shape[1] // wide
    for n in range(chunks):
        r, c = divmod(n, across)
        out_ref[n] = value[r * high : (r + 1) * high, c * wide : (c + 1) * wide]


def heads_kernel(y_ref, w_ref, out_ref, x, scr):
    chunks, tall, wide = y_ref.shape
    across = x.shape[1] // wide
    for n in range(chunks):
        r, c = divmod(n, across)
        x[r * tall : (r + 1) * tall, c * wide : (c + 1) * wide] = y_ref[n]
    members, high, lanes = out_ref.shape
    rows = x.shape[0]
    each = rows // members
    squares = jnp.sum(jnp.square(x[...].astype(jnp.float32)), axis=1, keepdims=True)
    scr[:rows, :lanes] = jnp.dot(x[...], w_ref[...], preferred_element_type=jnp.float32)
    scr[:rows, lanes:] = jnp.broadcast_to(squares, (rows, 128))
    row = lax.broadcasted_iota(jnp.int32, (high, 128), 0)
    lane = lax.broadcasted_iota(jnp.int32, (high, 128), 1)
    for k in range(members):
        piece = scr[k * each : k * each + high, :]
        line = jnp.sum(jnp.where((row == lane) & (row < each), piece[:, lanes:], 0.0), axis=0, keepdims=True)
        out_ref[k, :, :128] = jnp.where(row < each, piece[:, :128], line).astype(jnp.bfloat16)
        out_ref[k, :, 128:] = piece[:, 128:lanes].astype(jnp.bfloat16)


def paired_weights(norm_gain, w_gate, w_up):
    p = lax.axis_index("kvp")
    both = jnp.stack([w.T.reshape(2, -1, w.shape[0]) for w in (w_gate, w_up)], axis=1)
    both = (both.astype(jnp.float32) * norm_gain).astype(jnp.bfloat16)
    got = lax.ppermute(mine(both, 1 - p), "kvp", [(0, 1), (1, 0)])
    return mine(both, p), got


def feed_forward(gathered, weights, w_down, flat):
    own_w, got_w = weights
    members = lax.axis_size("kvh")
    wide, part = own_w.shape[2], own_w.shape[1]
    rows = gathered.size // (2 * wide)
    tall, half = rows // members, -(-(part + 1) // 128) * 128
    sent = local_call(
        up_kernel,
        jax.ShapeDtypeStruct((members, tall, 2 * half), jnp.bfloat16),
        gathered,
        own_w,
        got_w,
        scratch=(pltpu.VMEM((2, rows, wide), jnp.bfloat16),),
        flops=8 * rows * wide * part,
    )
    total = exchange(sent, "kvh").astype(jnp.float32).sum(axis=0)
    features = wide * lax.axis_size(KV)
    factor = lax.rsqrt(total[:, part : part + 1] / features + EPS_NORM)
    hidden = jax.nn.silu(factor * total[:, :part]) * (factor * total[:, half : half + part])
    everyone = spread(hidden.astype(jnp.bfloat16), KV)
    width = w_down.shape[1]
    shape = (rows, width) if flat else (lax.axis_size("tp"), tall, 2 * rows * width // (lax.axis_size("tp") * 2 * tall))
    return local_call(
        down_kernel,
        jax.ShapeDtypeStruct(shape, jnp.bfloat16),
        everyone,
        w_down,
        scratch=(pltpu.VMEM((rows, part), jnp.bfloat16),),
        flops=4 * rows * part * width,
    )


def advance(own, back, branch):
    share = exchange(back, "tp").astype(jnp.float32).sum(axis=0)
    return (own.astype(jnp.float32) + branch * share).astype(jnp.bfloat16)


def rotate(values_in, cosine, sine):
    half = values_in.shape[-1] // 2
    low, high = values_in[..., :half], values_in[..., half:]
    return jnp.concatenate([low * cosine - high * sine, low * sine + high * cosine], axis=-1)


def retention(gathered, w_heads, features, head_gain, state, tables):
    cosine, sine, decays = tables
    count, heads, width, _ = state.shape
    members = lax.axis_size(KV)
    chunks, tall, wide = gathered.shape
    block, lanes = w_heads.shape
    rows = members * count
    high = -(-(count + 1) // 8) * 8
    sent = local_call(
        heads_kernel,
        jax.ShapeDtypeStruct((members, high, lanes), jnp.bfloat16),
        gathered,
        w_heads,
        scratch=(
            pltpu.VMEM((rows, block), jnp.bfloat16),
            pltpu.VMEM((rows + 8, lanes + 128), jnp.float32),
        ),
        flops=2 * rows * block * lanes,
    )
    total = exchange(sent, KV).astype(jnp.float32).sum(axis=0)
    factor = lax.rsqrt(total[count, :count] / features + EPS_NORM)[:, None]
    total = factor * total[:count]
    q, k, v, o = (total[:, i * heads * width : (i + 1) * heads * width].reshape(count, heads, width) for i in range(4))
    q = rotate(q, cosine, sine)
    k = rotate(k, cosine, sine) * width ** (-0.5)
    carried = jnp.einsum("shd,shde->she", q, state, precision=lax.Precision.HIGHEST)
    within = jnp.sum(q * k, axis=-1, keepdims=True)
    mixture = decays[None, :, None] * carried + within * v
    centered = mixture - jnp.mean(mixture, axis=-1, keepdims=True)
    variance = jnp.mean(centered * centered, axis=-1, keepdims=True)
    normed = centered * lax.rsqrt(variance + EPS_GROUP) * head_gain.reshape(heads, width)
    ret_out = (jax.nn.silu(o) * normed).astype(jnp.bfloat16).reshape(count, heads * width)
    new_state = decays[None, :, None, None] * state + k[..., :, None] * v[..., None, :]
    return spread(ret_out, KV).reshape(rows, heads * width), new_state


def per_device(
    stream_in,
    positions,
    ret_state,
    first_gain,
    first_gate,
    first_up,
    first_down,
    mix_gain,
    w_query,
    w_key,
    w_value,
    w_outgate,
    w_out,
    head_gain,
    second_gain,
    second_gate,
    second_up,
    second_down,
):
    few, block = stream_in.shape
    tp, t, p = lax.axis_size("tp"), lax.axis_index("tp"), lax.axis_index("kvp")
    features = block * lax.axis_size(KV)
    rows = few * tp
    groups = lax.axis_size("kvh")
    tall, across = rows // groups, tp // groups
    wide = block // across

    half = ret_state.shape[-1] // 2
    inverse = 10000.0 ** (-jnp.arange(half, dtype=jnp.float32) / half)
    angles = positions.astype(jnp.float32)[:, None] * inverse[None, :]
    cosine, sine = jnp.cos(angles)[:, None, :], jnp.sin(angles)[:, None, :]
    heads = ret_state.shape[1]
    head_ids = (t * heads + jnp.arange(heads)).astype(jnp.float32)
    decays = jnp.exp(jnp.log1p(-(2.0 ** (-5.0 - head_ids))))

    first_pair = paired_weights(first_gain, first_gate, first_up)
    second_pair = paired_weights(second_gain, second_gate, second_up)
    w_heads = jnp.concatenate([w_query, w_key, w_value, w_outgate], axis=1)
    w_heads = (w_heads.astype(jnp.float32) * mix_gain[:, None]).astype(jnp.bfloat16)

    gathered = spread(stream_in, BOTH).reshape(2, rows, block)
    own = lax.dynamic_slice(gathered, (p, (t // across) * tall, (t % across) * wide), (1, tall, wide))[0]
    back = feed_forward(gathered, first_pair, first_down, False)
    own = advance(own, back, 0.5)
    gathered = spread(own, "tp")
    ret_out, new_state = retention(
        gathered, w_heads, features, head_gain, ret_state, (cosine, sine, decays)
    )
    back = jnp.dot(ret_out, w_out, preferred_element_type=jnp.float32).astype(jnp.bfloat16)
    back = back.reshape(groups, tall, across, wide).transpose(0, 2, 1, 3).reshape(tp, tall, wide)
    own = advance(own, back, 1.0)
    gathered = spread(own, BOTH).reshape(2, tp, tall, wide)
    place = (t * few) // tall
    own = lax.dynamic_slice(
        gathered, (p, place * across, t * few - place * tall, 0), (1, across, few, wide)
    )[0]
    own = jnp.concatenate([own[c] for c in range(across)], axis=1)
    back = feed_forward(gathered, second_pair, second_down, True)
    return advance(own, back.reshape(tp, few, block), 0.5), new_state


def solution(mesh):
    sizes = dict(mesh.shape)
    shape = (sizes["grp"], sizes["kv"] // 2, 2, sizes["tp"])
    fine = Mesh(np.asarray(mesh.devices).reshape(shape), ("grp", *KV, "tp"))
    rows, tall, flat = P(("grp", "tp"), KV), P(KV, "tp"), P("tp", KV)
    in_specs = (
        rows,
        P(("grp", *KV)),
        P(("grp", *KV), "tp", None, None),
        P(KV),
        tall,
        tall,
        flat,
        P(KV),
        tall,
        tall,
        tall,
        tall,
        flat,
        P("tp"),
        P(KV),
        tall,
        tall,
        flat,
    )
    out_specs = (rows, P(("grp", *KV), "tp", None, None))
    return jax.shard_map(
        per_device, mesh=fine, in_specs=in_specs, out_specs=out_specs, check_vma=False
    )
```

```python
import jax
import jax.numpy as jnp
import numpy as np
from jax import lax
from jax.experimental import pallas as pl
from jax.experimental.pallas import tpu as pltpu
from jax.sharding import Mesh
from jax.sharding import PartitionSpec as P

EPS_NORM = 1e-06
EPS_GROUP = 1e-05
KV = ("kvh", "kvp")
BOTH = ("kvp", "tp")
VMEM = pl.BlockSpec(memory_space=pltpu.VMEM)
NT = (((1,), (1,)), ((), ()))


def local_call(kernel, out_shape, *args, scratch=(), flops=0):
    return pl.pallas_call(
        kernel,
        out_shape=out_shape,
        in_specs=[VMEM] * len(args),
        out_specs=jax.tree.map(lambda _: VMEM, out_shape),
        scratch_shapes=scratch,
        cost_estimate=pl.CostEstimate(flops=flops, bytes_accessed=2**20, transcendentals=0),
        compiler_params=pltpu.CompilerParams(vmem_limit_bytes=16 * 2**20),
    )(*args)


def exchange(x, axis):
    return lax.all_to_all(x, axis, split_axis=0, concat_axis=0, tiled=True)


def spread(x, axis):
    return exchange(jnp.broadcast_to(x[None], (lax.axis_size(axis), *x.shape)), axis)


def mine(x, index):
    return lax.dynamic_index_in_dim(x, index, 0, keepdims=False)


def fill_rows(x, y_ref, p):
    if len(y_ref.shape) == 3:
        x[0] = y_ref[p]
        x[1] = y_ref[1 - p]
        return
    _, chunks, tall, wide = y_ref.shape
    across = x.shape[2] // wide
    for n in range(chunks):
        r, c = divmod(n, across)
        place = (slice(r * tall, (r + 1) * tall), slice(c * wide, (c + 1) * wide))
        x[(0, *place)] = y_ref[p, n]
        x[(1, *place)] = y_ref[1 - p, n]


def up_kernel(y_ref, own_ref, got_ref, out_ref, x):
    fill_rows(x, y_ref, lax.axis_index("kvp"))
    groups, tall, lanes = out_ref.shape
    part = own_ref.shape[1]
    half = lanes // 2
    squares = sum(jnp.sum(jnp.square(x[j].astype(jnp.float32)), axis=1, keepdims=True) for j in range(2))
    for i in range(2):
        value = sum(
            lax.dot_general(x[j], w[i], NT, preferred_element_type=jnp.float32)
            for j, w in enumerate((own_ref, got_ref))
        )
        rows = jnp.concatenate([value, jnp.broadcast_to(squares, (value.shape[0], half - part))], axis=1)
        rows = rows.astype(jnp.bfloat16)
        for r in range(groups):
            out_ref[r, :, i * half : (i + 1) * half] = rows[r * tall : (r + 1) * tall]


def down_kernel(h_ref, own_ref, got_ref, out_ref, h):
    groups, tall, _ = h_ref.shape
    p = lax.axis_index("kvp")
    for r in range(groups):
        h[r * tall : (r + 1) * tall] = h_ref[r]
    for place, w in ((p, own_ref), (1 - p, got_ref)):
        value = jnp.dot(h[...], w[2], preferred_element_type=jnp.float32).astype(jnp.bfloat16)
        if len(out_ref.shape) == 3:
            out_ref[place] = value
            continue
        _, chunks, high, wide = out_ref.shape
        across = value.shape[1] // wide
        for n in range(chunks):
            r, c = divmod(n, across)
            out_ref[place, n] = value[r * high : (r + 1) * high, c * wide : (c + 1) * wide]


def heads_kernel(y_ref, own_ref, got_ref, out_ref, x, scr):
    fill_rows(x, y_ref, lax.axis_index("kvp"))
    members, high, lanes = out_ref.shape
    rows = x.shape[1]
    each = rows // members
    squares = sum(jnp.sum(jnp.square(x[j].astype(jnp.float32)), axis=1, keepdims=True) for j in range(2))
    scr[:rows, :lanes] = sum(
        jnp.dot(x[j], w[...], preferred_element_type=jnp.float32) for j, w in enumerate((own_ref, got_ref))
    )
    scr[:rows, lanes:] = jnp.broadcast_to(squares, (rows, 128))
    scr[rows:] = jnp.zeros((scr.shape[0] - rows, scr.shape[1]), jnp.float32)
    row = lax.broadcasted_iota(jnp.int32, (high, 128), 0)
    lane = lax.broadcasted_iota(jnp.int32, (high, 128), 1)
    for k in range(members):
        piece = scr[k * each : k * each + high, :]
        line = jnp.sum(jnp.where((row == lane) & (row < each), piece[:, lanes:], 0.0), axis=0, keepdims=True)
        out_ref[k, :, :128] = jnp.where(row < each, piece[:, :128], line).astype(jnp.bfloat16)
        out_ref[k, :, 128:] = piece[:, 128:lanes].astype(jnp.bfloat16)


def swapped(both):
    p = lax.axis_index("kvp")
    return mine(both, p), lax.ppermute(mine(both, 1 - p), "kvp", [(0, 1), (1, 0)])


def paired_weights(norm_gain, w_gate, w_up, w_down):
    width = w_gate.shape[0]
    scaled = [(w.T.astype(jnp.float32) * norm_gain).astype(jnp.bfloat16) for w in (w_gate, w_up)]
    return swapped(jnp.stack([w.reshape(2, -1, width) for w in (*scaled, w_down)], axis=1))


def feed_forward(gathered, weights, flat):
    own_w, got_w = weights
    members, tp = lax.axis_size("kvh"), lax.axis_size("tp")
    wide, part = own_w.shape[2], own_w.shape[1]
    rows = gathered.size // (2 * wide)
    tall, half = rows // members, -(-(part + 1) // 128) * 128
    sent = local_call(
        up_kernel,
        jax.ShapeDtypeStruct((members, tall, 2 * half), jnp.bfloat16),
        gathered,
        own_w,
        got_w,
        scratch=(pltpu.VMEM((2, rows, wide), jnp.bfloat16),),
        flops=8 * rows * wide * part,
    )
    total = exchange(sent, "kvh").astype(jnp.float32).sum(axis=0)
    features = wide * lax.axis_size(KV)
    factor = lax.rsqrt(total[:, part : part + 1] / features + EPS_NORM)
    hidden = jax.nn.silu(factor * total[:, :part]) * (factor * total[:, half : half + part])
    everyone = spread(hidden.astype(jnp.bfloat16), "kvh")
    shape = (2, rows, wide) if flat else (2, tp, tall, rows * wide // (tp * tall))
    return local_call(
        down_kernel,
        jax.ShapeDtypeStruct(shape, jnp.bfloat16),
        everyone,
        own_w,
        got_w,
        scratch=(pltpu.VMEM((rows, part), jnp.bfloat16),),
        flops=4 * rows * part * wide,
    )


def advance(own, back, branch, axis):
    share = exchange(back, axis).astype(jnp.float32).sum(axis=0)
    return (own.astype(jnp.float32) + branch * share).astype(jnp.bfloat16)


def rotate(values_in, cosine, sine):
    half = values_in.shape[-1] // 2
    low, high = values_in[..., :half], values_in[..., half:]
    return jnp.concatenate([low * cosine - high * sine, low * sine + high * cosine], axis=-1)


def retention(gathered, weights, features, head_gain, state, tables):
    cosine, sine, decays = tables
    count, heads, width, _ = state.shape
    members = lax.axis_size(KV)
    block, lanes = weights[0].shape
    rows = members * count
    high = -(-(count + 1) // 8) * 8
    sent = local_call(
        heads_kernel,
        jax.ShapeDtypeStruct((members, high, lanes), jnp.bfloat16),
        gathered,
        *weights,
        scratch=(
            pltpu.VMEM((2, rows, block), jnp.bfloat16),
            pltpu.VMEM((rows + 8, lanes + 128), jnp.float32),
        ),
        flops=4 * rows * block * lanes,
    )
    total = exchange(sent, KV).reshape(members // 2, 2, high, lanes).astype(jnp.float32).sum(axis=0)
    factor = lax.rsqrt(total[0, count, :count] / features + EPS_NORM)[:, None]
    total = factor * total[:, :count]
    wide = heads * width
    q, k, v, o = (
        total[i // 2, :, i % 2 * wide : (i % 2 + 1) * wide].reshape(count, heads, width) for i in range(4)
    )
    q = rotate(q, cosine, sine)
    k = rotate(k, cosine, sine) * width ** (-0.5)
    carried = jnp.einsum("shd,shde->she", q, state, precision=lax.Precision.HIGHEST)
    within = jnp.sum(q * k, axis=-1, keepdims=True)
    mixture = decays[None, :, None] * carried + within * v
    centered = mixture - jnp.mean(mixture, axis=-1, keepdims=True)
    variance = jnp.mean(centered * centered, axis=-1, keepdims=True)
    normed = centered * lax.rsqrt(variance + EPS_GROUP) * head_gain.reshape(heads, width)
    ret_out = (jax.nn.silu(o) * normed).astype(jnp.bfloat16).reshape(count, heads * width)
    new_state = decays[None, :, None, None] * state + k[..., :, None] * v[..., None, :]
    return spread(ret_out, KV).reshape(rows, heads * width), new_state


def per_device(
    stream_in,
    positions,
    ret_state,
    first_gain,
    first_gate,
    first_up,
    first_down,
    mix_gain,
    w_query,
    w_key,
    w_value,
    w_outgate,
    w_out,
    head_gain,
    second_gain,
    second_gate,
    second_up,
    second_down,
):
    few, block = stream_in.shape
    tp, t, p = lax.axis_size("tp"), lax.axis_index("tp"), lax.axis_index("kvp")
    features = block * lax.axis_size(KV)
    rows = few * tp
    groups = lax.axis_size("kvh")
    tall, across = rows // groups, tp // groups
    wide = block // across
    r, c = lax.div(t, across), lax.rem(t, across)

    half = ret_state.shape[-1] // 2
    inverse = 10000.0 ** (-jnp.arange(half, dtype=jnp.float32) / half)
    angles = positions.astype(jnp.float32)[:, None] * inverse[None, :]
    cosine, sine = jnp.cos(angles)[:, None, :], jnp.sin(angles)[:, None, :]
    heads = ret_state.shape[1]
    head_ids = (t * heads + jnp.arange(heads)).astype(jnp.float32)
    decays = jnp.exp(jnp.log1p(-(2.0 ** (-5.0 - head_ids))))
    tables = (cosine, sine, decays)

    first_pair = paired_weights(first_gain, first_gate, first_up, first_down)
    second_pair = paired_weights(second_gain, second_gate, second_up, second_down)
    halves = [jnp.concatenate(w, axis=1) for w in ((w_query, w_key), (w_value, w_outgate))]
    halves = jnp.stack(halves).astype(jnp.float32) * mix_gain[:, None]
    heads_pair = swapped(halves.astype(jnp.bfloat16))

    gathered = spread(stream_in, BOTH).reshape(2, rows, block)
    own = lax.dynamic_slice(gathered, (p, r * tall, c * wide), (1, tall, wide))[0]
    gathered, own, tables = lax.optimization_barrier((gathered, own, tables))
    back = feed_forward(gathered, first_pair, False)
    own = advance(own, back.reshape(2 * tp, tall, wide), 0.5, BOTH)
    gathered = spread(own, BOTH).reshape(2, tp, tall, wide)
    ret_out, new_state = retention(gathered, heads_pair, features, head_gain, ret_state, tables)
    back = jnp.dot(ret_out, w_out, preferred_element_type=jnp.float32).astype(jnp.bfloat16)
    back = back.reshape(groups, tall, across, wide).transpose(0, 2, 1, 3).reshape(tp, tall, wide)
    own = advance(own, back, 1.0, "tp")
    gathered = spread(own, BOTH).reshape(2, tp, tall, wide)
    place = lax.div(t * few, tall)
    own = lax.dynamic_slice(gathered, (p, place * across, t * few - place * tall, 0), (1, across, few, wide))[0]
    own = jnp.concatenate([own[i] for i in range(across)], axis=1)
    gathered, own = lax.optimization_barrier((gathered, own))
    back = feed_forward(gathered, second_pair, True)
    return advance(own, back.reshape(2 * tp, few, block), 0.5, BOTH), new_state


def solution(mesh):
    sizes = dict(mesh.shape)
    shape = (sizes["grp"], sizes["kv"] // 2, 2, sizes["tp"])
    fine = Mesh(np.asarray(mesh.devices).reshape(shape), ("grp", *KV, "tp"))
    rows, tall, flat = P(("grp", "tp"), KV), P(KV, "tp"), P("tp", KV)
    in_specs = (
        rows,
        P(("grp", *KV)),
        P(("grp", *KV), "tp", None, None),
        P(KV),
        tall,
        tall,
        flat,
        P(KV),
        tall,
        tall,
        tall,
        tall,
        flat,
        P("tp"),
        P(KV),
        tall,
        tall,
        flat,
    )
    out_specs = (rows, P(("grp", *KV), "tp", None, None))
    return jax.shard_map(per_device, mesh=fine, in_specs=in_specs, out_specs=out_specs, check_vma=False)
```

```python
import functools

import jax
import jax.numpy as jnp
import numpy as np
from jax import lax
from jax.experimental import pallas as pl
from jax.experimental.pallas import tpu as pltpu
from jax.sharding import Mesh
from jax.sharding import PartitionSpec as P

EPS_NORM = 1e-06
EPS_GROUP = 1e-05
KV = ("kvh", "kvp")
BOTH = ("kvp", "tp")
VMEM = pl.BlockSpec(memory_space=pltpu.VMEM)
NT = (((1,), (1,)), ((), ()))


def local_call(kernel, out_shape, *args, scratch=(), flops=0):
    return pl.pallas_call(
        kernel,
        out_shape=out_shape,
        in_specs=[VMEM] * len(args),
        out_specs=jax.tree.map(lambda _: VMEM, out_shape),
        scratch_shapes=scratch,
        cost_estimate=pl.CostEstimate(flops=flops, bytes_accessed=2**20, transcendentals=0),
        compiler_params=pltpu.CompilerParams(vmem_limit_bytes=16 * 2**20),
    )(*args)


def exchange(x, axis):
    return lax.all_to_all(x, axis, split_axis=0, concat_axis=0, tiled=True)


def spread(x, axis):
    return exchange(jnp.broadcast_to(x[None], (lax.axis_size(axis), *x.shape)), axis)


def mine(x, index):
    return lax.dynamic_index_in_dim(x, index, 0, keepdims=False)


def fill_rows(x, y_ref, p):
    if len(y_ref.shape) == 3:
        x[0] = y_ref[p]
        x[1] = y_ref[1 - p]
        return
    _, chunks, tall, wide = y_ref.shape
    across = x.shape[2] // wide
    for n in range(chunks):
        r, c = divmod(n, across)
        place = (slice(r * tall, (r + 1) * tall), slice(c * wide, (c + 1) * wide))
        x[(0, *place)] = y_ref[p, n]
        x[(1, *place)] = y_ref[1 - p, n]


def up_kernel(y_ref, own_ref, got_ref, out_ref, x):
    fill_rows(x, y_ref, lax.axis_index("kvp"))
    groups, tall, lanes = out_ref.shape
    part = own_ref.shape[1]
    half = lanes // 2
    squares = sum(jnp.sum(jnp.square(x[j].astype(jnp.float32)), axis=1, keepdims=True) for j in range(2))
    for i in range(2):
        value = sum(
            lax.dot_general(x[j], w[i], NT, preferred_element_type=jnp.float32)
            for j, w in enumerate((own_ref, got_ref))
        )
        rows = jnp.concatenate([value, jnp.broadcast_to(squares, (value.shape[0], half - part))], axis=1)
        rows = rows.astype(jnp.bfloat16)
        for r in range(groups):
            out_ref[r, :, i * half : (i + 1) * half] = rows[r * tall : (r + 1) * tall]


def down_kernel(h_ref, own_ref, got_ref, out_ref, h, scr):
    groups, tall, _ = h_ref.shape
    p = lax.axis_index("kvp")
    for r in range(groups):
        h[r * tall : (r + 1) * tall] = h_ref[r]
    _, chunks, high, wide = out_ref.shape
    across = scr.shape[1] // wide
    for place, w in ((p, own_ref), (1 - p, got_ref)):
        scr[...] = jnp.dot(h[...], w[...], preferred_element_type=jnp.float32)
        for n in range(chunks):
            r, c = divmod(n, across)
            piece = scr[r * high : (r + 1) * high, c * wide : (c + 1) * wide]
            out_ref[place, n] = piece.astype(jnp.bfloat16)


def heads_kernel(y_ref, own_ref, got_ref, out_ref, x, scr):
    fill_rows(x, y_ref, lax.axis_index("kvp"))
    members, high, lanes = out_ref.shape
    rows = x.shape[1]
    each = rows // members
    squares = sum(jnp.sum(jnp.square(x[j].astype(jnp.float32)), axis=1, keepdims=True) for j in range(2))
    scr[:rows, :lanes] = sum(
        jnp.dot(x[j], w[...], preferred_element_type=jnp.float32) for j, w in enumerate((own_ref, got_ref))
    )
    scr[:rows, lanes:] = jnp.broadcast_to(squares, (rows, 128))
    scr[rows:] = jnp.zeros((scr.shape[0] - rows, scr.shape[1]), jnp.float32)
    row = lax.broadcasted_iota(jnp.int32, (high, 128), 0)
    lane = lax.broadcasted_iota(jnp.int32, (high, 128), 1)
    for k in range(members):
        piece = scr[k * each : k * each + high, :]
        line = jnp.sum(jnp.where((row == lane) & (row < each), piece[:, lanes:], 0.0), axis=0, keepdims=True)
        out_ref[k, :, :128] = jnp.where(row < each, piece[:, :128], line).astype(jnp.bfloat16)
        out_ref[k, :, 128:] = piece[:, 128:lanes].astype(jnp.bfloat16)


def retention_kernel(features, z_ref, state_ref, cos_ref, sin_ref, decay_ref, gain_ref, out_ref, k_ref, v_ref):
    members, high, _ = z_ref.shape
    count, width = k_ref.shape
    left, right = (
        sum(z_ref[n].astype(jnp.float32) for n in range(start, members, 2)) for start in range(2)
    )
    row = lax.broadcasted_iota(jnp.int32, (high, width), 0)
    lane = lax.broadcasted_iota(jnp.int32, (high, width), 1)
    line = jnp.broadcast_to(left[count : count + 1, :width], (high, width))
    squares = jnp.sum(jnp.where((row == lane) & (row < count), line, 0.0), axis=1, keepdims=True)
    factor = lax.rsqrt(squares / features + EPS_NORM)
    q, k, v, o = (factor * part for part in (left[:, :width], left[:, width:], right[:, :width], right[:, width:]))
    q, k, v, o = (part[:count] for part in (q, k, v, o))
    cosine, sine = cos_ref[...], sin_ref[...]
    q = q * cosine + pltpu.roll(q, width // 2, 1) * sine
    k = (k * cosine + pltpu.roll(k, width // 2, 1) * sine) * width ** (-0.5)
    k_ref[...] = k
    v_ref[...] = v
    square = jnp.concatenate([q, jnp.zeros((width - count, width), jnp.float32)], axis=0).T
    carried = jnp.concatenate(
        [jnp.sum(square[:, s : s + 1] * state_ref[s], axis=0, keepdims=True) for s in range(count)], axis=0
    )
    within = jnp.sum(q * k, axis=1, keepdims=True)
    mixture = decay_ref[...] * carried + within * v
    centered = mixture - jnp.mean(mixture, axis=1, keepdims=True)
    variance = jnp.mean(centered * centered, axis=1, keepdims=True)
    normed = centered * lax.rsqrt(variance + EPS_GROUP) * gain_ref[...]
    value = (o / (1.0 + jnp.exp(-o)) * normed).astype(jnp.bfloat16)
    for n in range(members):
        out_ref[n] = value


def swapped(both):
    p = lax.axis_index("kvp")
    return mine(both, p), lax.ppermute(mine(both, 1 - p), "kvp", [(0, 1), (1, 0)])


def paired_weights(norm_gain, w_gate, w_up):
    width = w_gate.shape[0]
    scaled = [(w.T.astype(jnp.float32) * norm_gain).astype(jnp.bfloat16) for w in (w_gate, w_up)]
    return swapped(jnp.stack([w.reshape(2, -1, width) for w in scaled], axis=1))


def paired_rows(w_down):
    return swapped(w_down.reshape(2, -1, w_down.shape[1]))


def feed_forward(gathered, weights, back_weights, flat):
    own_w, got_w = weights
    members, tp = lax.axis_size("kvh"), lax.axis_size("tp")
    wide, part = own_w.shape[2], own_w.shape[1]
    rows = gathered.size // (2 * wide)
    tall, half = rows // members, -(-(part + 1) // 128) * 128
    sent = local_call(
        up_kernel,
        jax.ShapeDtypeStruct((members, tall, 2 * half), jnp.bfloat16),
        gathered,
        own_w,
        got_w,
        scratch=(pltpu.VMEM((2, rows, wide), jnp.bfloat16),),
        flops=8 * rows * wide * part,
    )
    total = exchange(sent, "kvh").astype(jnp.float32).sum(axis=0)
    features = wide * lax.axis_size(KV)
    factor = lax.rsqrt(total[:, part : part + 1] / features + EPS_NORM)
    hidden = jax.nn.silu(factor * total[:, :part]) * (factor * total[:, half : half + part])
    hidden, back_weights = lax.optimization_barrier((hidden.astype(jnp.bfloat16), back_weights))
    everyone = spread(hidden, "kvh")
    shape = (2, tp, rows // tp, wide) if flat else (2, tp, tall, rows * wide // (tp * tall))
    return local_call(
        down_kernel,
        jax.ShapeDtypeStruct(shape, jnp.bfloat16),
        everyone,
        *back_weights,
        scratch=(pltpu.VMEM((rows, part), jnp.bfloat16), pltpu.VMEM((rows, wide), jnp.float32)),
        flops=4 * rows * part * wide,
    )


def advance(own, back, branch, axis):
    share = exchange(back, axis).astype(jnp.float32).sum(axis=0)
    return (own.astype(jnp.float32) + branch * share).astype(jnp.bfloat16)


def retention(gathered, weights, features, head_gain, state, tables):
    cosine, sine, decay = tables
    count, _, width, _ = state.shape
    members = lax.axis_size(KV)
    block, lanes = weights[0].shape
    rows = members * count
    high = -(-(count + 1) // 8) * 8
    sent = local_call(
        heads_kernel,
        jax.ShapeDtypeStruct((members, high, lanes), jnp.bfloat16),
        gathered,
        *weights,
        scratch=(
            pltpu.VMEM((2, rows, block), jnp.bfloat16),
            pltpu.VMEM((rows + 8, lanes + 128), jnp.float32),
        ),
        flops=4 * rows * block * lanes,
    )
    received = exchange(sent, KV)
    ret_out, k, v = local_call(
        functools.partial(retention_kernel, features),
        (
            jax.ShapeDtypeStruct((members, count, width), jnp.bfloat16),
            jax.ShapeDtypeStruct((count, width), jnp.float32),
            jax.ShapeDtypeStruct((count, width), jnp.float32),
        ),
        received,
        state.reshape(count, width, width),
        cosine,
        sine,
        decay,
        head_gain.reshape(1, width),
        flops=4 * count * width * width,
    )
    new_state = decay[:, :, None] * state.reshape(count, width, width) + k[:, :, None] * v[:, None, :]
    return exchange(ret_out, KV).reshape(rows, width), new_state.reshape(state.shape)


def per_device(
    stream_in,
    positions,
    ret_state,
    first_gain,
    first_gate,
    first_up,
    first_down,
    mix_gain,
    w_query,
    w_key,
    w_value,
    w_outgate,
    w_out,
    head_gain,
    second_gain,
    second_gate,
    second_up,
    second_down,
):
    few, block = stream_in.shape
    tp, t, p = lax.axis_size("tp"), lax.axis_index("tp"), lax.axis_index("kvp")
    features = block * lax.axis_size(KV)
    rows = few * tp
    groups = lax.axis_size("kvh")
    tall, across = rows // groups, tp // groups
    wide = block // across
    r, c = lax.div(t, across), lax.rem(t, across)

    half = ret_state.shape[-1] // 2
    inverse = 10000.0 ** (-jnp.arange(half, dtype=jnp.float32) / half)
    angles = positions.astype(jnp.float32)[:, None] * inverse[None, :]
    cosine, sine = jnp.cos(angles), jnp.sin(angles)
    cosine, sine = jnp.concatenate([cosine, cosine], axis=1), jnp.concatenate([-sine, sine], axis=1)
    decay = jnp.exp(jnp.log1p(-(2.0 ** (-5.0 - t.astype(jnp.float32))))) * jnp.ones((1, 2 * half), jnp.float32)
    place = lax.div(t * few, tall)
    ready = (cosine, sine, decay, place, t * few - place * tall)

    first_pair = paired_weights(first_gain, first_gate, first_up)
    first_back = paired_rows(first_down)
    second_pair = paired_weights(second_gain, second_gate, second_up)
    second_back = paired_rows(second_down)
    halves = [jnp.concatenate(w, axis=1) for w in ((w_query, w_key), (w_value, w_outgate))]
    halves = jnp.stack(halves).astype(jnp.float32) * mix_gain[:, None]
    heads_pair = swapped(halves.astype(jnp.bfloat16))

    gathered = spread(stream_in, BOTH).reshape(2, rows, block)
    own = lax.dynamic_slice(gathered, (p, r * tall, c * wide), (1, tall, wide))[0]
    gathered, own, ready = lax.optimization_barrier((gathered, own, ready))
    cosine, sine, decay, place, offset = ready
    back = feed_forward(gathered, first_pair, first_back, False)
    own = advance(own, back.reshape(2 * tp, tall, wide), 0.5, BOTH)
    gathered = spread(own, BOTH).reshape(2, tp, tall, wide)
    ret_out, new_state = retention(gathered, heads_pair, features, head_gain, ret_state, (cosine, sine, decay))
    back = jnp.dot(ret_out, w_out, preferred_element_type=jnp.float32).astype(jnp.bfloat16)
    back = back.reshape(groups, tall, across, wide).transpose(0, 2, 1, 3).reshape(tp, tall, wide)
    own = advance(own, back, 1.0, "tp")
    gathered = spread(own, BOTH).reshape(2, tp, tall, wide)
    own = lax.dynamic_slice(gathered, (p, place * across, offset, 0), (1, across, few, wide))[0]
    own = jnp.concatenate([own[i] for i in range(across)], axis=1)
    gathered, own = lax.optimization_barrier((gathered, own))
    back = feed_forward(gathered, second_pair, second_back, True)
    return advance(own, back.reshape(2 * tp, few, block), 0.5, BOTH), new_state


def solution(mesh):
    sizes = dict(mesh.shape)
    shape = (sizes["grp"], sizes["kv"] // 2, 2, sizes["tp"])
    fine = Mesh(np.asarray(mesh.devices).reshape(shape), ("grp", *KV, "tp"))
    rows, tall, flat = P(("grp", "tp"), KV), P(KV, "tp"), P("tp", KV)
    in_specs = (
        rows,
        P(("grp", *KV)),
        P(("grp", *KV), "tp", None, None),
        P(KV),
        tall,
        tall,
        flat,
        P(KV),
        tall,
        tall,
        tall,
        tall,
        flat,
        P("tp"),
        P(KV),
        tall,
        tall,
        flat,
    )
    out_specs = (rows, P(("grp", *KV), "tp", None, None))
    return jax.shard_map(per_device, mesh=fine, in_specs=in_specs, out_specs=out_specs, check_vma=False)
```

```python
import functools

import jax
import jax.numpy as jnp
import numpy as np
from jax import lax
from jax.experimental import pallas as pl
from jax.experimental.pallas import tpu as pltpu
from jax.sharding import Mesh
from jax.sharding import PartitionSpec as P

EPS_NORM = 1e-06
EPS_GROUP = 1e-05
KV = ("kvh", "kvp")
BOTH = ("kvp", "tp")
VMEM = pl.BlockSpec(memory_space=pltpu.VMEM)
NT = (((1,), (1,)), ((), ()))


def local_call(kernel, out_shape, *args, scratch=(), flops=0):
    return pl.pallas_call(
        kernel,
        out_shape=out_shape,
        in_specs=[VMEM] * len(args),
        out_specs=jax.tree.map(lambda _: VMEM, out_shape),
        scratch_shapes=scratch,
        cost_estimate=pl.CostEstimate(flops=flops, bytes_accessed=2**20, transcendentals=0),
        compiler_params=pltpu.CompilerParams(vmem_limit_bytes=16 * 2**20),
    )(*args)


def exchange(x, axis):
    return lax.all_to_all(x, axis, split_axis=0, concat_axis=0, tiled=True)


def spread(x, axis):
    return exchange(jnp.broadcast_to(x[None], (lax.axis_size(axis), *x.shape)), axis)


def mine(x, index):
    return lax.dynamic_index_in_dim(x, index, 0, keepdims=False)


def fill_rows(x, y_ref, p):
    if len(y_ref.shape) == 3:
        x[0] = y_ref[p]
        x[1] = y_ref[1 - p]
        return
    _, chunks, tall, wide = y_ref.shape
    across = x.shape[2] // wide
    for n in range(chunks):
        r, c = divmod(n, across)
        place = (slice(r * tall, (r + 1) * tall), slice(c * wide, (c + 1) * wide))
        x[(0, *place)] = y_ref[p, n]
        x[(1, *place)] = y_ref[1 - p, n]


def up_kernel(y_ref, own_ref, got_ref, out_ref, x):
    fill_rows(x, y_ref, lax.axis_index("kvp"))
    groups, tall, lanes = out_ref.shape
    part = own_ref.shape[1]
    half = lanes // 2
    squares = sum(jnp.sum(jnp.square(x[j].astype(jnp.float32)), axis=1, keepdims=True) for j in range(2))
    for i in range(2):
        value = sum(
            lax.dot_general(x[j], w[i], NT, preferred_element_type=jnp.float32)
            for j, w in enumerate((own_ref, got_ref))
        )
        rows = jnp.concatenate([value, jnp.broadcast_to(squares, (value.shape[0], half - part))], axis=1)
        rows = rows.astype(jnp.bfloat16)
        for r in range(groups):
            out_ref[r, :, i * half : (i + 1) * half] = rows[r * tall : (r + 1) * tall]


def down_kernel(h_ref, own_ref, got_ref, out_ref, h, scr):
    groups, tall, _ = h_ref.shape
    p = lax.axis_index("kvp")
    for r in range(groups):
        h[r * tall : (r + 1) * tall] = h_ref[r]
    _, chunks, high, wide = out_ref.shape
    across = scr.shape[1] // wide
    for place, w in ((p, own_ref), (1 - p, got_ref)):
        scr[...] = jnp.dot(h[...], w[...], preferred_element_type=jnp.float32)
        for n in range(chunks):
            r, c = divmod(n, across)
            piece = scr[r * high : (r + 1) * high, c * wide : (c + 1) * wide]
            out_ref[place, n] = piece.astype(jnp.bfloat16)


def whole_down_kernel(h_ref, w_ref, out_ref, h, scr):
    groups, tall, part = h_ref.shape
    cuts = w_ref.shape[0] // part
    for c in range(cuts):
        for r in range(groups // cuts):
            h[c, r * tall : (r + 1) * tall] = h_ref[r * cuts + c]
    scr[...] = sum(
        jnp.dot(h[c], w_ref[c * part : (c + 1) * part], preferred_element_type=jnp.float32) for c in range(cuts)
    )
    chunks, high, wide = out_ref.shape
    across = scr.shape[1] // wide
    for n in range(chunks):
        r, c = divmod(n, across)
        piece = scr[r * high : (r + 1) * high, c * wide : (c + 1) * wide]
        out_ref[n] = piece.astype(jnp.bfloat16)


def heads_kernel(y_ref, own_ref, got_ref, out_ref, x, scr):
    fill_rows(x, y_ref, lax.axis_index("kvp"))
    members, high, lanes = out_ref.shape
    rows = x.shape[1]
    each = rows // members
    squares = sum(jnp.sum(jnp.square(x[j].astype(jnp.float32)), axis=1, keepdims=True) for j in range(2))
    scr[:rows, :lanes] = sum(
        jnp.dot(x[j], w[...], preferred_element_type=jnp.float32) for j, w in enumerate((own_ref, got_ref))
    )
    scr[:rows, lanes:] = jnp.broadcast_to(squares, (rows, 128))
    scr[rows:] = jnp.zeros((scr.shape[0] - rows, scr.shape[1]), jnp.float32)
    row = lax.broadcasted_iota(jnp.int32, (high, 128), 0)
    lane = lax.broadcasted_iota(jnp.int32, (high, 128), 1)
    for k in range(members):
        piece = scr[k * each : k * each + high, :]
        line = jnp.sum(jnp.where((row == lane) & (row < each), piece[:, lanes:], 0.0), axis=0, keepdims=True)
        out_ref[k, :, :128] = jnp.where(row < each, piece[:, :128], line).astype(jnp.bfloat16)
        out_ref[k, :, 128:] = piece[:, 128:lanes].astype(jnp.bfloat16)


def retention_kernel(features, z_ref, state_ref, cos_ref, sin_ref, decay_ref, gain_ref, out_ref, k_ref, v_ref):
    members, high, _ = z_ref.shape
    count, width = k_ref.shape
    left, right = (
        sum(z_ref[n].astype(jnp.float32) for n in range(start, members, 2)) for start in range(2)
    )
    row = lax.broadcasted_iota(jnp.int32, (high, width), 0)
    lane = lax.broadcasted_iota(jnp.int32, (high, width), 1)
    line = jnp.broadcast_to(left[count : count + 1, :width], (high, width))
    squares = jnp.sum(jnp.where((row == lane) & (row < count), line, 0.0), axis=1, keepdims=True)
    factor = lax.rsqrt(squares / features + EPS_NORM)
    q, k, v, o = (factor * part for part in (left[:, :width], left[:, width:], right[:, :width], right[:, width:]))
    q, k, v, o = (part[:count] for part in (q, k, v, o))
    cosine, sine = cos_ref[...], sin_ref[...]
    q = q * cosine + pltpu.roll(q, width // 2, 1) * sine
    k = (k * cosine + pltpu.roll(k, width // 2, 1) * sine) * width ** (-0.5)
    k_ref[...] = k
    v_ref[...] = v
    square = jnp.concatenate([q, jnp.zeros((width - count, width), jnp.float32)], axis=0).T
    carried = jnp.concatenate(
        [jnp.sum(square[:, s : s + 1] * state_ref[s], axis=0, keepdims=True) for s in range(count)], axis=0
    )
    within = jnp.sum(q * k, axis=1, keepdims=True)
    mixture = decay_ref[...] * carried + within * v
    centered = mixture - jnp.mean(mixture, axis=1, keepdims=True)
    variance = jnp.mean(centered * centered, axis=1, keepdims=True)
    normed = centered * lax.rsqrt(variance + EPS_GROUP) * gain_ref[...]
    value = (o / (1.0 + jnp.exp(-o)) * normed).astype(jnp.bfloat16)
    for n in range(members):
        out_ref[n] = value


def swapped(both):
    p = lax.axis_index("kvp")
    return mine(both, p), lax.ppermute(mine(both, 1 - p), "kvp", [(0, 1), (1, 0)])


def paired_weights(norm_gain, w_gate, w_up):
    width = w_gate.shape[0]
    scaled = [(w.T.astype(jnp.float32) * norm_gain).astype(jnp.bfloat16) for w in (w_gate, w_up)]
    return swapped(jnp.stack([w.reshape(2, -1, width) for w in scaled], axis=1))


def paired_rows(w_down):
    return swapped(w_down.reshape(2, -1, w_down.shape[1]))


def feed_forward(gathered, weights, back_weights, flat):
    own_w, got_w = weights
    members, tp = lax.axis_size("kvh"), lax.axis_size("tp")
    wide, part = own_w.shape[2], own_w.shape[1]
    rows = gathered.size // (2 * wide)
    tall, half = rows // members, -(-(part + 1) // 128) * 128
    sent = local_call(
        up_kernel,
        jax.ShapeDtypeStruct((members, tall, 2 * half), jnp.bfloat16),
        gathered,
        own_w,
        got_w,
        scratch=(pltpu.VMEM((2, rows, wide), jnp.bfloat16),),
        flops=8 * rows * wide * part,
    )
    total = exchange(sent, "kvh").astype(jnp.float32).sum(axis=0)
    features = wide * lax.axis_size(KV)
    factor = lax.rsqrt(total[:, part : part + 1] / features + EPS_NORM)
    hidden = jax.nn.silu(factor * total[:, :part]) * (factor * total[:, half : half + part])
    hidden = hidden.astype(jnp.bfloat16)
    scratch = (pltpu.VMEM((rows, part), jnp.bfloat16), pltpu.VMEM((rows, wide), jnp.float32))
    if not flat:
        everyone = spread(hidden, KV)
        return local_call(
            whole_down_kernel,
            jax.ShapeDtypeStruct((tp, tall, rows * wide // (tp * tall)), jnp.bfloat16),
            everyone,
            back_weights,
            scratch=(pltpu.VMEM((2, rows, part), jnp.bfloat16), scratch[1]),
            flops=4 * rows * part * wide,
        )
    hidden, back_weights = lax.optimization_barrier((hidden, back_weights))
    everyone = spread(hidden, "kvh")
    return local_call(
        down_kernel,
        jax.ShapeDtypeStruct((2, tp, rows // tp, wide), jnp.bfloat16),
        everyone,
        *back_weights,
        scratch=scratch,
        flops=4 * rows * part * wide,
    )


def advance(own, back, branch, axis):
    share = exchange(back, axis).astype(jnp.float32).sum(axis=0)
    return (own.astype(jnp.float32) + branch * share).astype(jnp.bfloat16)


def retention(gathered, weights, features, head_gain, state, tables):
    cosine, sine, decay = tables
    count, _, width, _ = state.shape
    members = lax.axis_size(KV)
    block, lanes = weights[0].shape
    rows = members * count
    high = -(-(count + 1) // 8) * 8
    sent = local_call(
        heads_kernel,
        jax.ShapeDtypeStruct((members, high, lanes), jnp.bfloat16),
        gathered,
        *weights,
        scratch=(
            pltpu.VMEM((2, rows, block), jnp.bfloat16),
            pltpu.VMEM((rows + 8, lanes + 128), jnp.float32),
        ),
        flops=4 * rows * block * lanes,
    )
    received = exchange(sent, KV)
    ret_out, k, v = local_call(
        functools.partial(retention_kernel, features),
        (
            jax.ShapeDtypeStruct((members, count, width), jnp.bfloat16),
            jax.ShapeDtypeStruct((count, width), jnp.float32),
            jax.ShapeDtypeStruct((count, width), jnp.float32),
        ),
        received,
        state.reshape(count, width, width),
        cosine,
        sine,
        decay,
        head_gain.reshape(1, width),
        flops=4 * count * width * width,
    )
    new_state = decay[:, :, None] * state.reshape(count, width, width) + k[:, :, None] * v[:, None, :]
    return exchange(ret_out, KV).reshape(rows, width), new_state.reshape(state.shape)


def per_device(
    stream_in,
    positions,
    ret_state,
    first_gain,
    first_gate,
    first_up,
    first_down,
    mix_gain,
    w_query,
    w_key,
    w_value,
    w_outgate,
    w_out,
    head_gain,
    second_gain,
    second_gate,
    second_up,
    second_down,
):
    few, block = stream_in.shape
    tp, t, p = lax.axis_size("tp"), lax.axis_index("tp"), lax.axis_index("kvp")
    features = block * lax.axis_size(KV)
    rows = few * tp
    groups = lax.axis_size("kvh")
    tall, across = rows // groups, tp // groups
    wide = block // across
    r, c = lax.div(t, across), lax.rem(t, across)

    half = ret_state.shape[-1] // 2
    inverse = 10000.0 ** (-jnp.arange(half, dtype=jnp.float32) / half)
    angles = positions.astype(jnp.float32)[:, None] * inverse[None, :]
    cosine, sine = jnp.cos(angles), jnp.sin(angles)
    cosine, sine = jnp.concatenate([cosine, cosine], axis=1), jnp.concatenate([-sine, sine], axis=1)
    decay = jnp.exp(jnp.log1p(-(2.0 ** (-5.0 - t.astype(jnp.float32))))) * jnp.ones((1, 2 * half), jnp.float32)
    place = lax.div(t * few, tall)
    ready = (cosine, sine, decay, place, t * few - place * tall)

    first_pair = paired_weights(first_gain, first_gate, first_up)
    second_pair = paired_weights(second_gain, second_gate, second_up)
    second_back = paired_rows(second_down)
    halves = [jnp.concatenate(w, axis=1) for w in ((w_query, w_key), (w_value, w_outgate))]
    halves = jnp.stack(halves).astype(jnp.float32) * mix_gain[:, None]
    heads_pair = swapped(halves.astype(jnp.bfloat16))

    gathered = spread(stream_in, BOTH).reshape(2, rows, block)
    own = lax.dynamic_slice(gathered, (p, r * tall, c * wide), (1, tall, wide))[0]
    gathered, own, ready = lax.optimization_barrier((gathered, own, ready))
    cosine, sine, decay, place, offset = ready
    back = feed_forward(gathered, first_pair, first_down, False)
    own = advance(own, back, 0.5, "tp")
    gathered = spread(own, BOTH).reshape(2, tp, tall, wide)
    ret_out, new_state = retention(gathered, heads_pair, features, head_gain, ret_state, (cosine, sine, decay))
    back = jnp.dot(ret_out, w_out, preferred_element_type=jnp.float32).astype(jnp.bfloat16)
    back = back.reshape(groups, tall, across, wide).transpose(0, 2, 1, 3).reshape(tp, tall, wide)
    own = advance(own, back, 1.0, "tp")
    gathered = spread(own, BOTH).reshape(2, tp, tall, wide)
    own = lax.dynamic_slice(gathered, (p, place * across, offset, 0), (1, across, few, wide))[0]
    own = jnp.concatenate([own[i] for i in range(across)], axis=1)
    gathered, own = lax.optimization_barrier((gathered, own))
    back = feed_forward(gathered, second_pair, second_back, True)
    return advance(own, back.reshape(2 * tp, few, block), 0.5, BOTH), new_state


def solution(mesh):
    sizes = dict(mesh.shape)
    shape = (sizes["grp"], sizes["kv"] // 2, 2, sizes["tp"])
    fine = Mesh(np.asarray(mesh.devices).reshape(shape), ("grp", *KV, "tp"))
    rows, tall, flat = P(("grp", "tp"), KV), P(KV, "tp"), P("tp", KV)
    in_specs = (
        rows,
        P(("grp", *KV)),
        P(("grp", *KV), "tp", None, None),
        P(KV),
        tall,
        tall,
        flat,
        P(KV),
        tall,
        tall,
        tall,
        tall,
        flat,
        P("tp"),
        P(KV),
        tall,
        tall,
        flat,
    )
    out_specs = (rows, P(("grp", *KV), "tp", None, None))
    return jax.shard_map(per_device, mesh=fine, in_specs=in_specs, out_specs=out_specs, check_vma=False)
```

```python
import functools

import jax
import jax.numpy as jnp
import numpy as np
from jax import lax
from jax.experimental import pallas as pl
from jax.experimental.pallas import tpu as pltpu
from jax.sharding import Mesh
from jax.sharding import PartitionSpec as P

EPS_NORM = 1e-06
EPS_GROUP = 1e-05
KV = ("kvh", "kvp")
BOTH = ("kvp", "tp")
VMEM = pl.BlockSpec(memory_space=pltpu.VMEM)
NT = (((1,), (1,)), ((), ()))


def local_call(kernel, out_shape, *args, scratch=(), flops=0):
    return pl.pallas_call(
        kernel,
        out_shape=out_shape,
        in_specs=[VMEM] * len(args),
        out_specs=jax.tree.map(lambda _: VMEM, out_shape),
        scratch_shapes=scratch,
        cost_estimate=pl.CostEstimate(flops=flops, bytes_accessed=2**20, transcendentals=0),
        compiler_params=pltpu.CompilerParams(vmem_limit_bytes=16 * 2**20),
    )(*args)


def exchange(x, axis):
    return lax.all_to_all(x, axis, split_axis=0, concat_axis=0, tiled=True)


def spread(x, axis):
    return exchange(jnp.broadcast_to(x[None], (lax.axis_size(axis), *x.shape)), axis)


def mine(x, index):
    return lax.dynamic_index_in_dim(x, index, 0, keepdims=False)


def fill_rows(x, y_ref, p):
    if len(y_ref.shape) == 3:
        x[0] = y_ref[p]
        x[1] = y_ref[1 - p]
        return
    _, chunks, tall, wide = y_ref.shape
    across = x.shape[2] // wide
    for n in range(chunks):
        r, c = divmod(n, across)
        place = (slice(r * tall, (r + 1) * tall), slice(c * wide, (c + 1) * wide))
        x[(0, *place)] = y_ref[p, n]
        x[(1, *place)] = y_ref[1 - p, n]


def up_kernel(y_ref, own_ref, got_ref, out_ref, x):
    fill_rows(x, y_ref, lax.axis_index("kvp"))
    groups, tall, lanes = out_ref.shape
    part = own_ref.shape[1]
    half = lanes // 2
    squares = sum(jnp.sum(jnp.square(x[j].astype(jnp.float32)), axis=1, keepdims=True) for j in range(2))
    for i in range(2):
        value = sum(
            lax.dot_general(x[j], w[i], NT, preferred_element_type=jnp.float32)
            for j, w in enumerate((own_ref, got_ref))
        )
        rows = jnp.concatenate([value, jnp.broadcast_to(squares, (value.shape[0], half - part))], axis=1)
        rows = rows.astype(jnp.bfloat16)
        for r in range(groups):
            out_ref[r, :, i * half : (i + 1) * half] = rows[r * tall : (r + 1) * tall]


def down_kernel(h_ref, own_ref, got_ref, out_ref, h, scr):
    groups, tall, _ = h_ref.shape
    p = lax.axis_index("kvp")
    for r in range(groups):
        h[r * tall : (r + 1) * tall] = h_ref[r]
    _, chunks, high, wide = out_ref.shape
    across = scr.shape[1] // wide
    for place, w in ((p, own_ref), (1 - p, got_ref)):
        scr[...] = jnp.dot(h[...], w[...], preferred_element_type=jnp.float32)
        for n in range(chunks):
            r, c = divmod(n, across)
            piece = scr[r * high : (r + 1) * high, c * wide : (c + 1) * wide]
            out_ref[place, n] = piece.astype(jnp.bfloat16)


def heads_kernel(y_ref, own_ref, got_ref, out_ref, x, scr):
    fill_rows(x, y_ref, lax.axis_index("kvp"))
    members, high, lanes = out_ref.shape
    rows = x.shape[1]
    each = rows // members
    squares = sum(jnp.sum(jnp.square(x[j].astype(jnp.float32)), axis=1, keepdims=True) for j in range(2))
    scr[:rows, :lanes] = sum(
        jnp.dot(x[j], w[...], preferred_element_type=jnp.float32) for j, w in enumerate((own_ref, got_ref))
    )
    scr[:rows, lanes:] = jnp.broadcast_to(squares, (rows, 128))
    scr[rows:] = jnp.zeros((scr.shape[0] - rows, scr.shape[1]), jnp.float32)
    row = lax.broadcasted_iota(jnp.int32, (high, 128), 0)
    lane = lax.broadcasted_iota(jnp.int32, (high, 128), 1)
    for k in range(members):
        piece = scr[k * each : k * each + high, :]
        line = jnp.sum(jnp.where((row == lane) & (row < each), piece[:, lanes:], 0.0), axis=0, keepdims=True)
        out_ref[k, :, :128] = jnp.where(row < each, piece[:, :128], line).astype(jnp.bfloat16)
        out_ref[k, :, 128:] = piece[:, 128:lanes].astype(jnp.bfloat16)


def retention_kernel(features, z_ref, state_ref, cos_ref, sin_ref, decay_ref, gain_ref, out_ref, k_ref, v_ref):
    members, high, _ = z_ref.shape
    count, width = k_ref.shape
    left, right = (
        sum(z_ref[n].astype(jnp.float32) for n in range(start, members, 2)) for start in range(2)
    )
    row = lax.broadcasted_iota(jnp.int32, (high, width), 0)
    lane = lax.broadcasted_iota(jnp.int32, (high, width), 1)
    line = jnp.broadcast_to(left[count : count + 1, :width], (high, width))
    squares = jnp.sum(jnp.where((row == lane) & (row < count), line, 0.0), axis=1, keepdims=True)
    factor = lax.rsqrt(squares / features + EPS_NORM)
    q, k, v, o = (factor * part for part in (left[:, :width], left[:, width:], right[:, :width], right[:, width:]))
    q, k, v, o = (part[:count] for part in (q, k, v, o))
    cosine, sine = cos_ref[...], sin_ref[...]
    q = q * cosine + pltpu.roll(q, width // 2, 1) * sine
    k = (k * cosine + pltpu.roll(k, width // 2, 1) * sine) * width ** (-0.5)
    k_ref[...] = k
    v_ref[...] = v
    square = jnp.concatenate([q, jnp.zeros((width - count, width), jnp.float32)], axis=0).T
    carried = jnp.concatenate(
        [jnp.sum(square[:, s : s + 1] * state_ref[s], axis=0, keepdims=True) for s in range(count)], axis=0
    )
    within = jnp.sum(q * k, axis=1, keepdims=True)
    mixture = decay_ref[...] * carried + within * v
    centered = mixture - jnp.mean(mixture, axis=1, keepdims=True)
    variance = jnp.mean(centered * centered, axis=1, keepdims=True)
    normed = centered * lax.rsqrt(variance + EPS_GROUP) * gain_ref[...]
    value = (o / (1.0 + jnp.exp(-o)) * normed).astype(jnp.bfloat16)
    for n in range(members):
        out_ref[n] = value


def swapped(both):
    p = lax.axis_index("kvp")
    return mine(both, p), lax.ppermute(mine(both, 1 - p), "kvp", [(0, 1), (1, 0)])


def paired_weights(norm_gain, w_gate, w_up):
    width = w_gate.shape[0]
    scaled = [(w.T.astype(jnp.float32) * norm_gain).astype(jnp.bfloat16) for w in (w_gate, w_up)]
    return swapped(jnp.stack([w.reshape(2, -1, width) for w in scaled], axis=1))


def paired_rows(w_down):
    return swapped(w_down.reshape(2, -1, w_down.shape[1]))


def feed_forward(gathered, weights, back_weights, flat):
    own_w, got_w = weights
    members, tp = lax.axis_size("kvh"), lax.axis_size("tp")
    wide, part = own_w.shape[2], own_w.shape[1]
    rows = gathered.size // (2 * wide)
    tall, half = rows // members, -(-(part + 1) // 128) * 128
    sent = local_call(
        up_kernel,
        jax.ShapeDtypeStruct((members, tall, 2 * half), jnp.bfloat16),
        gathered,
        own_w,
        got_w,
        scratch=(pltpu.VMEM((2, rows, wide), jnp.bfloat16),),
        flops=8 * rows * wide * part,
    )
    total = exchange(sent, "kvh").astype(jnp.float32).sum(axis=0)
    features = wide * lax.axis_size(KV)
    factor = lax.rsqrt(total[:, part : part + 1] / features + EPS_NORM)
    hidden = jax.nn.silu(factor * total[:, :part]) * (factor * total[:, half : half + part])
    hidden = hidden.astype(jnp.bfloat16)
    hidden, back_weights = lax.optimization_barrier((hidden, back_weights))
    everyone = spread(hidden, "kvh")
    chunk = (rows // tp, wide) if flat else (tall, rows * wide // (tp * tall))
    back = local_call(
        down_kernel,
        jax.ShapeDtypeStruct((2, tp, *chunk), jnp.bfloat16),
        everyone,
        *back_weights,
        scratch=(pltpu.VMEM((rows, part), jnp.bfloat16), pltpu.VMEM((rows, wide), jnp.float32)),
        flops=4 * rows * part * wide,
    )
    return back.reshape(2 * tp, *chunk)


def advance(own, back, branch, axis):
    share = exchange(back, axis).astype(jnp.float32).sum(axis=0)
    return (own.astype(jnp.float32) + branch * share).astype(jnp.bfloat16)


def retention(gathered, weights, features, head_gain, state, tables):
    cosine, sine, decay = tables
    count, _, width, _ = state.shape
    members = lax.axis_size(KV)
    block, lanes = weights[0].shape
    rows = members * count
    high = -(-(count + 1) // 8) * 8
    sent = local_call(
        heads_kernel,
        jax.ShapeDtypeStruct((members, high, lanes), jnp.bfloat16),
        gathered,
        *weights,
        scratch=(
            pltpu.VMEM((2, rows, block), jnp.bfloat16),
            pltpu.VMEM((rows + 8, lanes + 128), jnp.float32),
        ),
        flops=4 * rows * block * lanes,
    )
    received = exchange(sent, KV)
    ret_out, k, v = local_call(
        functools.partial(retention_kernel, features),
        (
            jax.ShapeDtypeStruct((members, count, width), jnp.bfloat16),
            jax.ShapeDtypeStruct((count, width), jnp.float32),
            jax.ShapeDtypeStruct((count, width), jnp.float32),
        ),
        received,
        state.reshape(count, width, width),
        cosine,
        sine,
        decay,
        head_gain.reshape(1, width),
        flops=4 * count * width * width,
    )
    new_state = decay[:, :, None] * state.reshape(count, width, width) + k[:, :, None] * v[:, None, :]
    return exchange(ret_out, KV).reshape(rows, width), new_state.reshape(state.shape)


def per_device(
    stream_in,
    positions,
    ret_state,
    first_gain,
    first_gate,
    first_up,
    first_down,
    mix_gain,
    w_query,
    w_key,
    w_value,
    w_outgate,
    w_out,
    head_gain,
    second_gain,
    second_gate,
    second_up,
    second_down,
):
    few, block = stream_in.shape
    tp, t, p = lax.axis_size("tp"), lax.axis_index("tp"), lax.axis_index("kvp")
    features = block * lax.axis_size(KV)
    rows = few * tp
    groups = lax.axis_size("kvh")
    tall, across = rows // groups, tp // groups
    wide = block // across
    r, c = lax.div(t, across), lax.rem(t, across)

    half = ret_state.shape[-1] // 2
    inverse = 10000.0 ** (-jnp.arange(half, dtype=jnp.float32) / half)
    angles = positions.astype(jnp.float32)[:, None] * inverse[None, :]
    cosine, sine = jnp.cos(angles), jnp.sin(angles)
    cosine, sine = jnp.concatenate([cosine, cosine], axis=1), jnp.concatenate([-sine, sine], axis=1)
    decay = jnp.exp(jnp.log1p(-(2.0 ** (-5.0 - t.astype(jnp.float32))))) * jnp.ones((1, 2 * half), jnp.float32)
    place = lax.div(t * few, tall)
    ready = (cosine, sine, decay, place, t * few - place * tall)

    first_pair = paired_weights(first_gain, first_gate, first_up)
    first_back = paired_rows(first_down)
    second_pair = paired_weights(second_gain, second_gate, second_up)
    second_back = paired_rows(second_down)
    halves = [jnp.concatenate(w, axis=1) for w in ((w_query, w_key), (w_value, w_outgate))]
    halves = jnp.stack(halves).astype(jnp.float32) * mix_gain[:, None]
    heads_pair = swapped(halves.astype(jnp.bfloat16))

    gathered = spread(stream_in, BOTH).reshape(2, rows, block)
    own = lax.dynamic_slice(gathered, (p, r * tall, c * wide), (1, tall, wide))[0]
    gathered, own, ready = lax.optimization_barrier((gathered, own, ready))
    cosine, sine, decay, place, offset = ready
    back = feed_forward(gathered, first_pair, first_back, False)
    own = advance(own, back, 0.5, BOTH)
    gathered = spread(own, BOTH).reshape(2, tp, tall, wide)
    ret_out, new_state = retention(gathered, heads_pair, features, head_gain, ret_state, (cosine, sine, decay))
    back = jnp.dot(ret_out, w_out, preferred_element_type=jnp.float32).astype(jnp.bfloat16)
    back = back.reshape(groups, tall, across, wide).transpose(0, 2, 1, 3).reshape(tp, tall, wide)
    own = advance(own, back, 1.0, "tp")
    gathered = spread(own, BOTH).reshape(2, tp, tall, wide)
    own = lax.dynamic_slice(gathered, (p, place * across, offset, 0), (1, across, few, wide))[0]
    own = jnp.concatenate([own[i] for i in range(across)], axis=1)
    gathered, own = lax.optimization_barrier((gathered, own))
    back = feed_forward(gathered, second_pair, second_back, True)
    return advance(own, back, 0.5, BOTH), new_state


def solution(mesh):
    sizes = dict(mesh.shape)
    shape = (sizes["grp"], sizes["kv"] // 2, 2, sizes["tp"])
    fine = Mesh(np.asarray(mesh.devices).reshape(shape), ("grp", *KV, "tp"))
    rows, tall, flat = P(("grp", "tp"), KV), P(KV, "tp"), P("tp", KV)
    in_specs = (
        rows,
        P(("grp", *KV)),
        P(("grp", *KV), "tp", None, None),
        P(KV),
        tall,
        tall,
        flat,
        P(KV),
        tall,
        tall,
        tall,
        tall,
        flat,
        P("tp"),
        P(KV),
        tall,
        tall,
        flat,
    )
    out_specs = (rows, P(("grp", *KV), "tp", None, None))
    return jax.shard_map(per_device, mesh=fine, in_specs=in_specs, out_specs=out_specs, check_vma=False)
```

```python
import functools

import jax
import jax.numpy as jnp
import numpy as np
from jax import lax
from jax.experimental import pallas as pl
from jax.experimental.pallas import tpu as pltpu
from jax.sharding import Mesh
from jax.sharding import PartitionSpec as P

EPS_NORM = 1e-06
EPS_GROUP = 1e-05
KV = ("kvh", "kvp")
BOTH = ("kvp", "tp")
VMEM = pl.BlockSpec(memory_space=pltpu.VMEM)
NT = (((1,), (1,)), ((), ()))


def local_call(kernel, out_shape, *args, scratch=(), flops=0):
    return pl.pallas_call(
        kernel,
        out_shape=out_shape,
        in_specs=[VMEM] * len(args),
        out_specs=jax.tree.map(lambda _: VMEM, out_shape),
        scratch_shapes=scratch,
        cost_estimate=pl.CostEstimate(flops=flops, bytes_accessed=2**20, transcendentals=0),
        compiler_params=pltpu.CompilerParams(vmem_limit_bytes=16 * 2**20),
    )(*args)


def exchange(x, axis):
    return lax.all_to_all(x, axis, split_axis=0, concat_axis=0, tiled=True)


def spread(x, axis):
    return exchange(jnp.broadcast_to(x[None], (lax.axis_size(axis), *x.shape)), axis)


def mine(x, index):
    return lax.dynamic_index_in_dim(x, index, 0, keepdims=False)


def fill_rows(x, y_ref, p):
    _, chunks, tall, wide = y_ref.shape
    across = x.shape[2] // wide
    for n in range(chunks):
        r, c = divmod(n, across)
        place = (slice(r * tall, (r + 1) * tall), slice(c * wide, (c + 1) * wide))
        x[(0, *place)] = y_ref[p, n]
        x[(1, *place)] = y_ref[1 - p, n]


def fill_flat(x, y_ref, scr, p):
    _, chunks, tall, wide = y_ref.shape
    across = x.shape[2] // wide
    few = tall // across
    for j, q in enumerate((p, 1 - p)):
        for n in range(chunks):
            block = y_ref[q, n].astype(jnp.float32)
            for c in range(across):
                scr[n * few : (n + 1) * few, c * wide : (c + 1) * wide] = block[c * few : (c + 1) * few]
        x[j] = scr[...].astype(jnp.bfloat16)


def up_kernel(flat, y_ref, own_ref, got_ref, out_ref, x, scr):
    if flat:
        fill_flat(x, y_ref, scr, lax.axis_index("kvp"))
    else:
        fill_rows(x, y_ref, lax.axis_index("kvp"))
    groups, tall, lanes = out_ref.shape
    part = own_ref.shape[1]
    half = lanes // 2
    squares = sum(jnp.sum(jnp.square(x[j].astype(jnp.float32)), axis=1, keepdims=True) for j in range(2))
    for i in range(2):
        value = sum(
            lax.dot_general(x[j], w[i], NT, preferred_element_type=jnp.float32)
            for j, w in enumerate((own_ref, got_ref))
        )
        rows = jnp.concatenate([value, jnp.broadcast_to(squares, (value.shape[0], half - part))], axis=1)
        rows = rows.astype(jnp.bfloat16)
        for r in range(groups):
            out_ref[r, :, i * half : (i + 1) * half] = rows[r * tall : (r + 1) * tall]


def down_kernel(flat, h_ref, own_ref, got_ref, out_ref, h, scr):
    groups, tall, _ = h_ref.shape
    p = lax.axis_index("kvp")
    for r in range(groups):
        h[r * tall : (r + 1) * tall] = h_ref[r]
    _, chunks, high, wide = out_ref.shape
    across = scr.shape[1] // wide
    for place, w in ((p, own_ref), (1 - p, got_ref)):
        scr[...] = jnp.dot(h[...], w[...], preferred_element_type=jnp.float32)
        for n in range(chunks):
            if flat:
                few = high // across
                cuts = [scr[n * few : (n + 1) * few, c * wide : (c + 1) * wide] for c in range(across)]
                piece = jnp.concatenate(cuts, axis=0)
            else:
                r, c = divmod(n, across)
                piece = scr[r * high : (r + 1) * high, c * wide : (c + 1) * wide]
            out_ref[place, n] = piece.astype(jnp.bfloat16)


def heads_kernel(y_ref, own_ref, got_ref, out_ref, x, scr):
    fill_rows(x, y_ref, lax.axis_index("kvp"))
    members, high, lanes = out_ref.shape
    rows = x.shape[1]
    each = rows // members
    squares = sum(jnp.sum(jnp.square(x[j].astype(jnp.float32)), axis=1, keepdims=True) for j in range(2))
    scr[:rows, :lanes] = sum(
        jnp.dot(x[j], w[...], preferred_element_type=jnp.float32) for j, w in enumerate((own_ref, got_ref))
    )
    scr[:rows, lanes:] = jnp.broadcast_to(squares, (rows, 128))
    scr[rows:] = jnp.zeros((scr.shape[0] - rows, scr.shape[1]), jnp.float32)
    row = lax.broadcasted_iota(jnp.int32, (high, 128), 0)
    lane = lax.broadcasted_iota(jnp.int32, (high, 128), 1)
    for k in range(members):
        piece = scr[k * each : k * each + high, :]
        line = jnp.sum(jnp.where((row == lane) & (row < each), piece[:, lanes:], 0.0), axis=0, keepdims=True)
        out_ref[k, :, :128] = jnp.where(row < each, piece[:, :128], line).astype(jnp.bfloat16)
        out_ref[k, :, 128:] = piece[:, 128:lanes].astype(jnp.bfloat16)


def retention_kernel(features, z_ref, state_ref, cos_ref, sin_ref, decay_ref, gain_ref, out_ref, k_ref, v_ref):
    members, high, _ = z_ref.shape
    count, width = k_ref.shape
    left, right = (
        sum(z_ref[n].astype(jnp.float32) for n in range(start, members, 2)) for start in range(2)
    )
    row = lax.broadcasted_iota(jnp.int32, (high, width), 0)
    lane = lax.broadcasted_iota(jnp.int32, (high, width), 1)
    line = jnp.broadcast_to(left[count : count + 1, :width], (high, width))
    squares = jnp.sum(jnp.where((row == lane) & (row < count), line, 0.0), axis=1, keepdims=True)
    factor = lax.rsqrt(squares / features + EPS_NORM)
    q, k, v, o = (factor * part for part in (left[:, :width], left[:, width:], right[:, :width], right[:, width:]))
    q, k, v, o = (part[:count] for part in (q, k, v, o))
    cosine, sine = cos_ref[...], sin_ref[...]
    q = q * cosine + pltpu.roll(q, width // 2, 1) * sine
    k = (k * cosine + pltpu.roll(k, width // 2, 1) * sine) * width ** (-0.5)
    k_ref[...] = k
    v_ref[...] = v
    square = jnp.concatenate([q, jnp.zeros((width - count, width), jnp.float32)], axis=0).T
    carried = jnp.concatenate(
        [jnp.sum(square[:, s : s + 1] * state_ref[s], axis=0, keepdims=True) for s in range(count)], axis=0
    )
    within = jnp.sum(q * k, axis=1, keepdims=True)
    mixture = decay_ref[...] * carried + within * v
    centered = mixture - jnp.mean(mixture, axis=1, keepdims=True)
    variance = jnp.mean(centered * centered, axis=1, keepdims=True)
    normed = centered * lax.rsqrt(variance + EPS_GROUP) * gain_ref[...]
    value = (o / (1.0 + jnp.exp(-o)) * normed).astype(jnp.bfloat16)
    for n in range(members):
        out_ref[n] = value


def swapped(both):
    p = lax.axis_index("kvp")
    return mine(both, p), lax.ppermute(mine(both, 1 - p), "kvp", [(0, 1), (1, 0)])


def paired_weights(norm_gain, w_gate, w_up):
    p = lax.axis_index("kvp")
    halves = tuple(w.T.reshape(2, -1, w.shape[0]) for w in (w_gate, w_up))

    def scaled(index, halves):
        return jnp.stack([(mine(w, index).astype(jnp.float32) * norm_gain).astype(jnp.bfloat16) for w in halves])

    sent = scaled(1 - p, halves)
    sent, halves = lax.optimization_barrier((sent, halves))
    return scaled(p, halves), lax.ppermute(sent, "kvp", [(0, 1), (1, 0)])


def paired_rows(w_down):
    return swapped(w_down.reshape(2, -1, w_down.shape[1]))


def feed_forward(gathered, weights, back_weights, flat):
    own_w, got_w = weights
    members, tp = lax.axis_size("kvh"), lax.axis_size("tp")
    wide, part = own_w.shape[2], own_w.shape[1]
    rows = gathered.size // (2 * wide)
    tall, half = rows // members, -(-(part + 1) // 128) * 128
    sent = local_call(
        functools.partial(up_kernel, not flat),
        jax.ShapeDtypeStruct((members, tall, 2 * half), jnp.bfloat16),
        gathered,
        own_w,
        got_w,
        scratch=(pltpu.VMEM((2, rows, wide), jnp.bfloat16), pltpu.VMEM((rows, wide), jnp.float32)),
        flops=8 * rows * wide * part,
    )
    total = exchange(sent, "kvh").astype(jnp.float32).sum(axis=0)
    features = wide * lax.axis_size(KV)
    factor = lax.rsqrt(total[:, part : part + 1] / features + EPS_NORM)
    hidden = jax.nn.silu(factor * total[:, :part]) * (factor * total[:, half : half + part])
    hidden = hidden.astype(jnp.bfloat16)
    hidden, back_weights = lax.optimization_barrier((hidden, back_weights))
    everyone = spread(hidden, "kvh")
    chunk = (tall, rows * wide // (tp * tall))
    back = local_call(
        functools.partial(down_kernel, flat),
        jax.ShapeDtypeStruct((2, tp, *chunk), jnp.bfloat16),
        everyone,
        *back_weights,
        scratch=(pltpu.VMEM((rows, part), jnp.bfloat16), pltpu.VMEM((rows, wide), jnp.float32)),
        flops=4 * rows * part * wide,
    )
    return back.reshape(2 * tp, *chunk)


def advance(own, back, branch, axis):
    share = exchange(back, axis).astype(jnp.float32).sum(axis=0)
    if share.shape != own.shape:
        share = jnp.concatenate(jnp.split(share, own.shape[1] // share.shape[1], axis=0), axis=1)
    return (own.astype(jnp.float32) + branch * share).astype(jnp.bfloat16)


def retention(gathered, weights, features, head_gain, state, tables):
    cosine, sine, decay = tables
    count, _, width, _ = state.shape
    members = lax.axis_size(KV)
    block, lanes = weights[0].shape
    rows = members * count
    high = -(-(count + 1) // 8) * 8
    sent = local_call(
        heads_kernel,
        jax.ShapeDtypeStruct((members, high, lanes), jnp.bfloat16),
        gathered,
        *weights,
        scratch=(
            pltpu.VMEM((2, rows, block), jnp.bfloat16),
            pltpu.VMEM((rows + 8, lanes + 128), jnp.float32),
        ),
        flops=4 * rows * block * lanes,
    )
    received = exchange(sent, KV)
    ret_out, k, v = local_call(
        functools.partial(retention_kernel, features),
        (
            jax.ShapeDtypeStruct((members, count, width), jnp.bfloat16),
            jax.ShapeDtypeStruct((count, width), jnp.float32),
            jax.ShapeDtypeStruct((count, width), jnp.float32),
        ),
        received,
        state.reshape(count, width, width),
        cosine,
        sine,
        decay,
        head_gain.reshape(1, width),
        flops=4 * count * width * width,
    )
    new_state = decay[:, :, None] * state.reshape(count, width, width) + k[:, :, None] * v[:, None, :]
    return exchange(ret_out, KV).reshape(rows, width), new_state.reshape(state.shape)


def per_device(
    stream_in,
    positions,
    ret_state,
    first_gain,
    first_gate,
    first_up,
    first_down,
    mix_gain,
    w_query,
    w_key,
    w_value,
    w_outgate,
    w_out,
    head_gain,
    second_gain,
    second_gate,
    second_up,
    second_down,
):
    few, block = stream_in.shape
    tp, t, p = lax.axis_size("tp"), lax.axis_index("tp"), lax.axis_index("kvp")
    features = block * lax.axis_size(KV)
    rows = few * tp
    groups = lax.axis_size("kvh")
    tall, across = rows // groups, tp // groups
    wide = block // across
    r, c = lax.div(t, across), lax.rem(t, across)

    half = ret_state.shape[-1] // 2
    inverse = 10000.0 ** (-jnp.arange(half, dtype=jnp.float32) / half)
    angles = positions.astype(jnp.float32)[:, None] * inverse[None, :]
    cosine, sine = jnp.cos(angles), jnp.sin(angles)
    cosine, sine = jnp.concatenate([cosine, cosine], axis=1), jnp.concatenate([-sine, sine], axis=1)
    decay = jnp.exp(jnp.log1p(-(2.0 ** (-5.0 - t.astype(jnp.float32)))))
    place = lax.div(t * few, tall)
    scalars = (decay, place, t * few - place * tall)

    first_pair = paired_weights(first_gain, first_gate, first_up)
    first_back = paired_rows(first_down)
    second_back = paired_rows(second_down)
    halves = [jnp.concatenate(w, axis=1) for w in ((w_query, w_key), (w_value, w_outgate))]
    halves = jnp.stack(halves).astype(jnp.float32) * mix_gain[:, None]
    heads_pair = swapped(halves.astype(jnp.bfloat16))

    cuts = jnp.concatenate(jnp.split(stream_in, across, axis=1), axis=0)
    gathered = spread(cuts, BOTH).reshape(2, tp, tall, wide)
    own = lax.dynamic_slice(gathered, (p, r * across, c * few, 0), (1, across, few, wide)).reshape(tall, wide)
    gathered, own, scalars = lax.optimization_barrier((gathered, own, scalars))
    decay, place, offset = scalars
    back = feed_forward(gathered, first_pair, first_back, False)
    back, second_gain = lax.optimization_barrier((back, second_gain))
    second_pair = paired_weights(second_gain, second_gate, second_up)
    own = advance(own, back, 0.5, BOTH)
    gathered = spread(own, BOTH).reshape(2, tp, tall, wide)
    gathered, cosine, sine = lax.optimization_barrier((gathered, cosine, sine))
    decay = jnp.broadcast_to(decay, (1, 2 * half))
    ret_out, new_state = retention(gathered, heads_pair, features, head_gain, ret_state, (cosine, sine, decay))
    back = jnp.dot(ret_out, w_out, preferred_element_type=jnp.float32).astype(jnp.bfloat16)
    back = back.reshape(groups, tall, across, wide).transpose(0, 2, 1, 3).reshape(tp, tall, wide)
    own = advance(own, back, 1.0, "tp")
    gathered = spread(own, BOTH).reshape(2, tp, tall, wide)
    own = lax.dynamic_slice(gathered, (p, place * across, offset, 0), (1, across, few, wide))[0]
    own = jnp.concatenate([own[i] for i in range(across)], axis=1)
    gathered, own, scalars = lax.optimization_barrier((gathered, own, scalars))
    decay, place, offset = scalars
    back = feed_forward(gathered, second_pair, second_back, True)
    return advance(own, back, 0.5, BOTH), new_state


def solution(mesh):
    sizes = dict(mesh.shape)
    shape = (sizes["grp"], sizes["kv"] // 2, 2, sizes["tp"])
    fine = Mesh(np.asarray(mesh.devices).reshape(shape), ("grp", *KV, "tp"))
    rows, tall, flat = P(("grp", "tp"), KV), P(KV, "tp"), P("tp", KV)
    in_specs = (
        rows,
        P(("grp", *KV)),
        P(("grp", *KV), "tp", None, None),
        P(KV),
        tall,
        tall,
        flat,
        P(KV),
        tall,
        tall,
        tall,
        tall,
        flat,
        P("tp"),
        P(KV),
        tall,
        tall,
        flat,
    )
    out_specs = (rows, P(("grp", *KV), "tp", None, None))
    return jax.shard_map(per_device, mesh=fine, in_specs=in_specs, out_specs=out_specs, check_vma=False)
```

```python
import functools

import jax
import jax.numpy as jnp
import numpy as np
from jax import lax
from jax.experimental import pallas as pl
from jax.experimental.pallas import tpu as pltpu
from jax.sharding import Mesh
from jax.sharding import PartitionSpec as P

EPS_NORM = 1e-06
EPS_GROUP = 1e-05
KV = ("kvh", "kvp")
BOTH = ("kvp", "tp")
VMEM = pl.BlockSpec(memory_space=pltpu.VMEM)
NT = (((1,), (1,)), ((), ()))


def local_call(kernel, out_shape, *args, scratch=(), flops=0):
    return pl.pallas_call(
        kernel,
        out_shape=out_shape,
        in_specs=[VMEM] * len(args),
        out_specs=jax.tree.map(lambda _: VMEM, out_shape),
        scratch_shapes=scratch,
        cost_estimate=pl.CostEstimate(flops=flops, bytes_accessed=2**20, transcendentals=0),
        compiler_params=pltpu.CompilerParams(vmem_limit_bytes=16 * 2**20),
    )(*args)


def exchange(x, axis):
    return lax.all_to_all(x, axis, split_axis=0, concat_axis=0, tiled=True)


def spread(x, axis):
    return exchange(jnp.broadcast_to(x[None], (lax.axis_size(axis), *x.shape)), axis)


def mine(x, index):
    return lax.dynamic_index_in_dim(x, index, 0, keepdims=False)


def fill_rows(x, y_ref, p):
    _, chunks, tall, wide = y_ref.shape
    across = x.shape[2] // wide
    for n in range(chunks):
        r, c = divmod(n, across)
        place = (slice(r * tall, (r + 1) * tall), slice(c * wide, (c + 1) * wide))
        x[(0, *place)] = y_ref[p, n]
        x[(1, *place)] = y_ref[1 - p, n]


def fill_flat(x, y_ref, scr, p):
    _, chunks, tall, wide = y_ref.shape
    across = x.shape[2] // wide
    few = tall // across
    for j, q in enumerate((p, 1 - p)):
        for n in range(chunks):
            block = y_ref[q, n].astype(jnp.float32)
            for c in range(across):
                scr[n * few : (n + 1) * few, c * wide : (c + 1) * wide] = block[c * few : (c + 1) * few]
        x[j] = scr[...].astype(jnp.bfloat16)


def up_kernel(flat, y_ref, own_ref, got_ref, out_ref, x, scr):
    if flat:
        fill_flat(x, y_ref, scr, lax.axis_index("kvp"))
    else:
        fill_rows(x, y_ref, lax.axis_index("kvp"))
    groups, tall, lanes = out_ref.shape
    part = own_ref.shape[1]
    half = lanes // 2
    squares = sum(jnp.sum(jnp.square(x[j].astype(jnp.float32)), axis=1, keepdims=True) for j in range(2))
    for i in range(2):
        value = sum(
            lax.dot_general(x[j], w[i], NT, preferred_element_type=jnp.float32)
            for j, w in enumerate((own_ref, got_ref))
        )
        rows = jnp.concatenate([value, jnp.broadcast_to(squares, (value.shape[0], half - part))], axis=1)
        rows = rows.astype(jnp.bfloat16)
        for r in range(groups):
            out_ref[r, :, i * half : (i + 1) * half] = rows[r * tall : (r + 1) * tall]


def down_kernel(flat, h_ref, own_ref, got_ref, out_ref, h, scr):
    groups, tall, _ = h_ref.shape
    p = lax.axis_index("kvp")
    for r in range(groups):
        h[r * tall : (r + 1) * tall] = h_ref[r]
    _, chunks, high, wide = out_ref.shape
    across = scr.shape[1] // wide
    for place, w in ((p, own_ref), (1 - p, got_ref)):
        scr[...] = jnp.dot(h[...], w[...], preferred_element_type=jnp.float32)
        for n in range(chunks):
            if flat:
                few = high // across
                cuts = [scr[n * few : (n + 1) * few, c * wide : (c + 1) * wide] for c in range(across)]
                piece = jnp.concatenate(cuts, axis=0)
            else:
                r, c = divmod(n, across)
                piece = scr[r * high : (r + 1) * high, c * wide : (c + 1) * wide]
            out_ref[place, n] = piece.astype(jnp.bfloat16)


def heads_kernel(y_ref, own_ref, got_ref, out_ref, x, scr):
    fill_rows(x, y_ref, lax.axis_index("kvp"))
    members, high, lanes = out_ref.shape
    rows = x.shape[1]
    each = rows // members
    squares = sum(jnp.sum(jnp.square(x[j].astype(jnp.float32)), axis=1, keepdims=True) for j in range(2))
    scr[:rows, :lanes] = sum(
        jnp.dot(x[j], w[...], preferred_element_type=jnp.float32) for j, w in enumerate((own_ref, got_ref))
    )
    scr[:rows, lanes:] = jnp.broadcast_to(squares, (rows, 128))
    scr[rows:] = jnp.zeros((scr.shape[0] - rows, scr.shape[1]), jnp.float32)
    row = lax.broadcasted_iota(jnp.int32, (high, 128), 0)
    lane = lax.broadcasted_iota(jnp.int32, (high, 128), 1)
    for k in range(members):
        piece = scr[k * each : k * each + high, :]
        line = jnp.sum(jnp.where((row == lane) & (row < each), piece[:, lanes:], 0.0), axis=0, keepdims=True)
        out_ref[k, :, :128] = jnp.where(row < each, piece[:, :128], line).astype(jnp.bfloat16)
        out_ref[k, :, 128:] = piece[:, 128:lanes].astype(jnp.bfloat16)


def retention_kernel(features, z_ref, state_ref, cos_ref, sin_ref, decay_ref, gain_ref, out_ref, k_ref, v_ref):
    members, high, _ = z_ref.shape
    count, width = k_ref.shape
    left, right = (
        sum(z_ref[n].astype(jnp.float32) for n in range(start, members, 2)) for start in range(2)
    )
    row = lax.broadcasted_iota(jnp.int32, (high, width), 0)
    lane = lax.broadcasted_iota(jnp.int32, (high, width), 1)
    line = jnp.broadcast_to(left[count : count + 1, :width], (high, width))
    squares = jnp.sum(jnp.where((row == lane) & (row < count), line, 0.0), axis=1, keepdims=True)
    factor = lax.rsqrt(squares / features + EPS_NORM)
    q, k, v, o = (factor * part for part in (left[:, :width], left[:, width:], right[:, :width], right[:, width:]))
    q, k, v, o = (part[:count] for part in (q, k, v, o))
    cosine, sine = cos_ref[...], sin_ref[...]
    q = q * cosine + pltpu.roll(q, width // 2, 1) * sine
    k = (k * cosine + pltpu.roll(k, width // 2, 1) * sine) * width ** (-0.5)
    k_ref[...] = k
    v_ref[...] = v
    square = jnp.concatenate([q, jnp.zeros((width - count, width), jnp.float32)], axis=0).T
    carried = jnp.concatenate(
        [jnp.sum(square[:, s : s + 1] * state_ref[s], axis=0, keepdims=True) for s in range(count)], axis=0
    )
    within = jnp.sum(q * k, axis=1, keepdims=True)
    mixture = decay_ref[...] * carried + within * v
    centered = mixture - jnp.mean(mixture, axis=1, keepdims=True)
    variance = jnp.mean(centered * centered, axis=1, keepdims=True)
    normed = centered * lax.rsqrt(variance + EPS_GROUP) * gain_ref[...]
    value = (o / (1.0 + jnp.exp(-o)) * normed).astype(jnp.bfloat16)
    for n in range(members):
        out_ref[n] = value


def swapped(both):
    p = lax.axis_index("kvp")
    return mine(both, p), lax.ppermute(mine(both, 1 - p), "kvp", [(0, 1), (1, 0)])


def paired_weights(norm_gain, w_gate, w_up):
    p = lax.axis_index("kvp")
    halves = tuple(w.T.reshape(2, -1, w.shape[0]) for w in (w_gate, w_up))

    def scaled(index, halves):
        return jnp.stack([(mine(w, index).astype(jnp.float32) * norm_gain).astype(jnp.bfloat16) for w in halves])

    sent = scaled(1 - p, halves)
    sent, halves = lax.optimization_barrier((sent, halves))
    return scaled(p, halves), lax.ppermute(sent, "kvp", [(0, 1), (1, 0)])


def paired_rows(w_down):
    return swapped(w_down.reshape(2, -1, w_down.shape[1]))


def feed_forward(gathered, weights, back_weights, flat):
    own_w, got_w = weights
    members, tp = lax.axis_size("kvh"), lax.axis_size("tp")
    wide, part = own_w.shape[2], own_w.shape[1]
    rows = gathered.size // (2 * wide)
    tall, half = rows // members, -(-(part + 1) // 128) * 128
    sent = local_call(
        functools.partial(up_kernel, not flat),
        jax.ShapeDtypeStruct((members, tall, 2 * half), jnp.bfloat16),
        gathered,
        own_w,
        got_w,
        scratch=(pltpu.VMEM((2, rows, wide), jnp.bfloat16), pltpu.VMEM((rows, wide), jnp.float32)),
        flops=8 * rows * wide * part,
    )
    total = exchange(sent, "kvh").astype(jnp.float32).sum(axis=0)
    features = wide * lax.axis_size(KV)
    factor = lax.rsqrt(total[:, part : part + 1] / features + EPS_NORM)
    hidden = jax.nn.silu(factor * total[:, :part]) * (factor * total[:, half : half + part])
    hidden = hidden.astype(jnp.bfloat16)
    hidden, back_weights = lax.optimization_barrier((hidden, back_weights))
    everyone = spread(hidden, "kvh")
    chunk = (tall, rows * wide // (tp * tall))
    back = local_call(
        functools.partial(down_kernel, flat),
        jax.ShapeDtypeStruct((2, tp, *chunk), jnp.bfloat16),
        everyone,
        *back_weights,
        scratch=(pltpu.VMEM((rows, part), jnp.bfloat16), pltpu.VMEM((rows, wide), jnp.float32)),
        flops=4 * rows * part * wide,
    )
    return back.reshape(2 * tp, *chunk)


def advance(own, back, branch, axis):
    share = exchange(back, axis).astype(jnp.float32).sum(axis=0)
    if share.shape != own.shape:
        share = jnp.concatenate(jnp.split(share, own.shape[1] // share.shape[1], axis=0), axis=1)
    return (own.astype(jnp.float32) + branch * share).astype(jnp.bfloat16)


def retention(gathered, weights, features, head_gain, state, tables):
    cosine, sine, decay = tables
    count, _, width, _ = state.shape
    members = lax.axis_size(KV)
    block, lanes = weights[0].shape
    rows = members * count
    high = -(-(count + 1) // 8) * 8
    sent = local_call(
        heads_kernel,
        jax.ShapeDtypeStruct((members, high, lanes), jnp.bfloat16),
        gathered,
        *weights,
        scratch=(
            pltpu.VMEM((2, rows, block), jnp.bfloat16),
            pltpu.VMEM((rows + 8, lanes + 128), jnp.float32),
        ),
        flops=4 * rows * block * lanes,
    )
    received = exchange(sent, KV)
    ret_out, k, v = local_call(
        functools.partial(retention_kernel, features),
        (
            jax.ShapeDtypeStruct((members, count, width), jnp.bfloat16),
            jax.ShapeDtypeStruct((count, width), jnp.float32),
            jax.ShapeDtypeStruct((count, width), jnp.float32),
        ),
        received,
        state.reshape(count, width, width),
        cosine,
        sine,
        decay,
        head_gain.reshape(1, width),
        flops=4 * count * width * width,
    )
    new_state = decay[:, :, None] * state.reshape(count, width, width) + k[:, :, None] * v[:, None, :]
    return exchange(ret_out, KV).reshape(rows, width), new_state.reshape(state.shape)


def per_device(
    stream_in,
    positions,
    ret_state,
    first_gain,
    first_gate,
    first_up,
    first_down,
    mix_gain,
    w_query,
    w_key,
    w_value,
    w_outgate,
    w_out,
    head_gain,
    second_gain,
    second_gate,
    second_up,
    second_down,
):
    few, block = stream_in.shape
    tp, t, p = lax.axis_size("tp"), lax.axis_index("tp"), lax.axis_index("kvp")
    features = block * lax.axis_size(KV)
    rows = few * tp
    groups = lax.axis_size("kvh")
    tall, across = rows // groups, tp // groups
    wide = block // across
    r, c = lax.div(t, across), lax.rem(t, across)

    half = ret_state.shape[-1] // 2
    inverse = 10000.0 ** (-jnp.arange(half, dtype=jnp.float32) / half)
    angles = positions.astype(jnp.float32)[:, None] * inverse[None, :]
    decay = jnp.exp(jnp.log1p(-(2.0 ** (-5.0 - t.astype(jnp.float32)))))
    place = lax.div(t * few, tall)
    early = (angles, decay, place, t * few - place * tall)

    first_pair = paired_weights(first_gain, first_gate, first_up)
    first_back = paired_rows(first_down)
    second_back = paired_rows(second_down)
    halves = [jnp.concatenate(w, axis=1) for w in ((w_query, w_key), (w_value, w_outgate))]
    halves = jnp.stack(halves).astype(jnp.float32) * mix_gain[:, None]
    heads_pair = swapped(halves.astype(jnp.bfloat16))

    cuts = jnp.concatenate(jnp.split(stream_in, across, axis=1), axis=0)
    gathered = spread(cuts, BOTH).reshape(2, tp, tall, wide)
    own = lax.dynamic_slice(gathered, (p, r * across, c * few, 0), (1, across, few, wide)).reshape(tall, wide)
    gathered, own, early = lax.optimization_barrier((gathered, own, early))
    angles, decay, place, offset = early
    back = feed_forward(gathered, first_pair, first_back, False)
    back, second_gain = lax.optimization_barrier((back, second_gain))
    second_pair = paired_weights(second_gain, second_gate, second_up)
    own = advance(own, back, 0.5, BOTH)
    gathered = spread(own, BOTH).reshape(2, tp, tall, wide)
    cosine, sine = jnp.cos(angles), jnp.sin(angles)
    cosine, sine = jnp.concatenate([cosine, cosine], axis=1), jnp.concatenate([-sine, sine], axis=1)
    gathered, cosine, sine = lax.optimization_barrier((gathered, cosine, sine))
    decay = jnp.broadcast_to(decay, (1, 2 * half))
    ret_out, new_state = retention(gathered, heads_pair, features, head_gain, ret_state, (cosine, sine, decay))
    back = jnp.dot(ret_out, w_out, preferred_element_type=jnp.float32).astype(jnp.bfloat16)
    back = back.reshape(groups, tall, across, wide).transpose(0, 2, 1, 3).reshape(tp, tall, wide)
    own = advance(own, back, 1.0, "tp")
    gathered = spread(own, BOTH).reshape(2, tp, tall, wide)
    own = lax.dynamic_slice(gathered, (p, place * across, offset, 0), (1, across, few, wide))[0]
    own = jnp.concatenate([own[i] for i in range(across)], axis=1)
    gathered, own, early = lax.optimization_barrier((gathered, own, early))
    angles, decay, place, offset = early
    back = feed_forward(gathered, second_pair, second_back, True)
    return advance(own, back, 0.5, BOTH), new_state


def solution(mesh):
    sizes = dict(mesh.shape)
    shape = (sizes["grp"], sizes["kv"] // 2, 2, sizes["tp"])
    fine = Mesh(np.asarray(mesh.devices).reshape(shape), ("grp", *KV, "tp"))
    rows, tall, flat = P(("grp", "tp"), KV), P(KV, "tp"), P("tp", KV)
    in_specs = (
        rows,
        P(("grp", *KV)),
        P(("grp", *KV), "tp", None, None),
        P(KV),
        tall,
        tall,
        flat,
        P(KV),
        tall,
        tall,
        tall,
        tall,
        flat,
        P("tp"),
        P(KV),
        tall,
        tall,
        flat,
    )
    out_specs = (rows, P(("grp", *KV), "tp", None, None))
    return jax.shard_map(per_device, mesh=fine, in_specs=in_specs, out_specs=out_specs, check_vma=False)
```

```python
import functools

import jax
import jax.numpy as jnp
import numpy as np
from jax import lax
from jax.experimental import pallas as pl
from jax.experimental.pallas import tpu as pltpu
from jax.sharding import Mesh
from jax.sharding import PartitionSpec as P

EPS_NORM = 1e-06
EPS_GROUP = 1e-05
KV = ("kvh", "kvp")
BOTH = ("kvp", "tp")
VMEM = pl.BlockSpec(memory_space=pltpu.VMEM)
NT = (((1,), (1,)), ((), ()))


def local_call(kernel, out_shape, *args, scratch=(), flops=0):
    return pl.pallas_call(
        kernel,
        out_shape=out_shape,
        in_specs=[VMEM] * len(args),
        out_specs=jax.tree.map(lambda _: VMEM, out_shape),
        scratch_shapes=scratch,
        cost_estimate=pl.CostEstimate(flops=flops, bytes_accessed=2**20, transcendentals=0),
        compiler_params=pltpu.CompilerParams(vmem_limit_bytes=16 * 2**20),
    )(*args)


def exchange(x, axis):
    return lax.all_to_all(x, axis, split_axis=0, concat_axis=0, tiled=True)


def spread(x, axis):
    return exchange(jnp.broadcast_to(x[None], (lax.axis_size(axis), *x.shape)), axis)


def mine(x, index):
    return lax.dynamic_index_in_dim(x, index, 0, keepdims=False)


def fill_rows(x, y_ref, p):
    _, chunks, tall, wide = y_ref.shape
    across = x.shape[2] // wide
    for n in range(chunks):
        r, c = divmod(n, across)
        place = (slice(r * tall, (r + 1) * tall), slice(c * wide, (c + 1) * wide))
        x[(0, *place)] = y_ref[p, n]
        x[(1, *place)] = y_ref[1 - p, n]


def fill_flat(x, y_ref, scr, p):
    _, chunks, tall, wide = y_ref.shape
    across = x.shape[2] // wide
    few = tall // across
    for j, q in enumerate((p, 1 - p)):
        for n in range(chunks):
            block = y_ref[q, n].astype(jnp.float32)
            for c in range(across):
                scr[n * few : (n + 1) * few, c * wide : (c + 1) * wide] = block[c * few : (c + 1) * few]
        x[j] = scr[...].astype(jnp.bfloat16)


def up_kernel(flat, y_ref, own_ref, got_ref, out_ref, x, scr):
    if flat:
        fill_flat(x, y_ref, scr, lax.axis_index("kvp"))
    else:
        fill_rows(x, y_ref, lax.axis_index("kvp"))
    groups, tall, lanes = out_ref.shape
    part = own_ref.shape[1]
    half = lanes // 2
    squares = sum(jnp.sum(jnp.square(x[j].astype(jnp.float32)), axis=1, keepdims=True) for j in range(2))
    for i in range(2):
        value = sum(
            lax.dot_general(x[j], w[i], NT, preferred_element_type=jnp.float32)
            for j, w in enumerate((own_ref, got_ref))
        )
        rows = jnp.concatenate([value, jnp.broadcast_to(squares, (value.shape[0], half - part))], axis=1)
        rows = rows.astype(jnp.bfloat16)
        for r in range(groups):
            out_ref[r, :, i * half : (i + 1) * half] = rows[r * tall : (r + 1) * tall]


def down_kernel(flat, h_ref, own_ref, got_ref, out_ref, h, scr):
    groups, tall, _ = h_ref.shape
    p = lax.axis_index("kvp")
    for r in range(groups):
        h[r * tall : (r + 1) * tall] = h_ref[r]
    _, chunks, high, wide = out_ref.shape
    across = scr.shape[1] // wide
    for place, w in ((p, own_ref), (1 - p, got_ref)):
        scr[...] = jnp.dot(h[...], w[: h.shape[1]], preferred_element_type=jnp.float32)
        for n in range(chunks):
            if flat:
                few = high // across
                cuts = [scr[n * few : (n + 1) * few, c * wide : (c + 1) * wide] for c in range(across)]
                piece = jnp.concatenate(cuts, axis=0)
            else:
                r, c = divmod(n, across)
                piece = scr[r * high : (r + 1) * high, c * wide : (c + 1) * wide]
            out_ref[place, n] = piece.astype(jnp.bfloat16)


def heads_kernel(y_ref, own_ref, got_ref, out_ref, x, scr):
    fill_rows(x, y_ref, lax.axis_index("kvp"))
    members, high, lanes = out_ref.shape
    rows = x.shape[1]
    each = rows // members
    squares = sum(jnp.sum(jnp.square(x[j].astype(jnp.float32)), axis=1, keepdims=True) for j in range(2))
    scr[:rows, :lanes] = sum(
        jnp.dot(x[j], w[w.shape[0] - x.shape[2] :], preferred_element_type=jnp.float32)
        for j, w in enumerate((own_ref, got_ref))
    )
    scr[:rows, lanes:] = jnp.broadcast_to(squares, (rows, 128))
    scr[rows:] = jnp.zeros((scr.shape[0] - rows, scr.shape[1]), jnp.float32)
    row = lax.broadcasted_iota(jnp.int32, (high, 128), 0)
    lane = lax.broadcasted_iota(jnp.int32, (high, 128), 1)
    for k in range(members):
        piece = scr[k * each : k * each + high, :]
        line = jnp.sum(jnp.where((row == lane) & (row < each), piece[:, lanes:], 0.0), axis=0, keepdims=True)
        out_ref[k, :, :128] = jnp.where(row < each, piece[:, :128], line).astype(jnp.bfloat16)
        out_ref[k, :, 128:] = piece[:, 128:lanes].astype(jnp.bfloat16)


def retention_kernel(features, z_ref, state_ref, cos_ref, sin_ref, decay_ref, gain_ref, out_ref, k_ref, v_ref):
    members, high, _ = z_ref.shape
    count, width = k_ref.shape
    left, right = (
        sum(z_ref[n].astype(jnp.float32) for n in range(start, members, 2)) for start in range(2)
    )
    row = lax.broadcasted_iota(jnp.int32, (high, width), 0)
    lane = lax.broadcasted_iota(jnp.int32, (high, width), 1)
    line = jnp.broadcast_to(left[count : count + 1, :width], (high, width))
    squares = jnp.sum(jnp.where((row == lane) & (row < count), line, 0.0), axis=1, keepdims=True)
    factor = lax.rsqrt(squares / features + EPS_NORM)
    q, k, v, o = (factor * part for part in (left[:, :width], left[:, width:], right[:, :width], right[:, width:]))
    q, k, v, o = (part[:count] for part in (q, k, v, o))
    cosine, sine = cos_ref[...], sin_ref[...]
    q = q * cosine + pltpu.roll(q, width // 2, 1) * sine
    k = (k * cosine + pltpu.roll(k, width // 2, 1) * sine) * width ** (-0.5)
    k_ref[...] = k
    v_ref[...] = v
    square = jnp.concatenate([q, jnp.zeros((width - count, width), jnp.float32)], axis=0).T
    carried = jnp.concatenate(
        [jnp.sum(square[:, s : s + 1] * state_ref[s], axis=0, keepdims=True) for s in range(count)], axis=0
    )
    within = jnp.sum(q * k, axis=1, keepdims=True)
    mixture = decay_ref[...] * carried + within * v
    centered = mixture - jnp.mean(mixture, axis=1, keepdims=True)
    variance = jnp.mean(centered * centered, axis=1, keepdims=True)
    normed = centered * lax.rsqrt(variance + EPS_GROUP) * gain_ref[...]
    value = (o / (1.0 + jnp.exp(-o)) * normed).astype(jnp.bfloat16)
    for n in range(members):
        out_ref[n] = value


def swapped(both):
    p = lax.axis_index("kvp")
    return mine(both, p), lax.ppermute(mine(both, 1 - p), "kvp", [(0, 1), (1, 0)])


def paired_weights(norm_gain, w_gate, w_up):
    p = lax.axis_index("kvp")
    halves = tuple(w.T.reshape(2, -1, w.shape[0]) for w in (w_gate, w_up))

    def scaled(index, halves):
        return jnp.stack([(mine(w, index).astype(jnp.float32) * norm_gain).astype(jnp.bfloat16) for w in halves])

    sent = scaled(1 - p, halves)
    sent, halves = lax.optimization_barrier((sent, halves))
    return scaled(p, halves), lax.ppermute(sent, "kvp", [(0, 1), (1, 0)])


def paired_rows(w_down):
    return swapped(w_down.reshape(2, -1, w_down.shape[1]))


def feed_forward(gathered, weights, back_weights, flat):
    own_w, got_w = weights
    members, tp = lax.axis_size("kvh"), lax.axis_size("tp")
    wide, part = own_w.shape[2], own_w.shape[1]
    rows = gathered.size // (2 * wide)
    tall, half = rows // members, -(-(part + 1) // 128) * 128
    sent = local_call(
        functools.partial(up_kernel, not flat),
        jax.ShapeDtypeStruct((members, tall, 2 * half), jnp.bfloat16),
        gathered,
        own_w,
        got_w,
        scratch=(pltpu.VMEM((2, rows, wide), jnp.bfloat16), pltpu.VMEM((rows, wide), jnp.float32)),
        flops=8 * rows * wide * part,
    )
    total = exchange(sent, "kvh").astype(jnp.float32).sum(axis=0)
    features = wide * lax.axis_size(KV)
    factor = lax.rsqrt(total[:, part : part + 1] / features + EPS_NORM)
    hidden = jax.nn.silu(factor * total[:, :part]) * (factor * total[:, half : half + part])
    hidden = hidden.astype(jnp.bfloat16)
    hidden, back_weights = lax.optimization_barrier((hidden, back_weights))
    everyone = spread(hidden, "kvh")
    chunk = (tall, rows * wide // (tp * tall))
    back = local_call(
        functools.partial(down_kernel, flat),
        jax.ShapeDtypeStruct((2, tp, *chunk), jnp.bfloat16),
        everyone,
        *back_weights,
        scratch=(pltpu.VMEM((rows, part), jnp.bfloat16), pltpu.VMEM((rows, wide), jnp.float32)),
        flops=4 * rows * part * wide,
    )
    return back.reshape(2 * tp, *chunk)


def advance(own, back, branch, axis):
    share = exchange(back, axis).astype(jnp.float32).sum(axis=0)
    if share.shape != own.shape:
        share = jnp.concatenate(jnp.split(share, own.shape[1] // share.shape[1], axis=0), axis=1)
    return (own.astype(jnp.float32) + branch * share).astype(jnp.bfloat16)


def retention(gathered, weights, features, head_gain, state, tables):
    cosine, sine, decay = tables
    count, _, width, _ = state.shape
    members = lax.axis_size(KV)
    lanes = weights[0].shape[1]
    rows = members * count
    block = gathered.size // (2 * rows)
    high = -(-(count + 1) // 8) * 8
    sent = local_call(
        heads_kernel,
        jax.ShapeDtypeStruct((members, high, lanes), jnp.bfloat16),
        gathered,
        *weights,
        scratch=(
            pltpu.VMEM((2, rows, block), jnp.bfloat16),
            pltpu.VMEM((rows + 8, lanes + 128), jnp.float32),
        ),
        flops=4 * rows * block * lanes,
    )
    received = exchange(sent, KV)
    ret_out, k, v = local_call(
        functools.partial(retention_kernel, features),
        (
            jax.ShapeDtypeStruct((members, count, width), jnp.bfloat16),
            jax.ShapeDtypeStruct((count, width), jnp.float32),
            jax.ShapeDtypeStruct((count, width), jnp.float32),
        ),
        received,
        state.reshape(count, width, width),
        cosine,
        sine,
        decay,
        head_gain.reshape(1, width),
        flops=4 * count * width * width,
    )
    new_state = decay[:, :, None] * state.reshape(count, width, width) + k[:, :, None] * v[:, None, :]
    return exchange(ret_out, KV).reshape(rows, width), new_state.reshape(state.shape)


def per_device(
    stream_in,
    positions,
    ret_state,
    first_gain,
    first_gate,
    first_up,
    first_down,
    mix_gain,
    w_query,
    w_key,
    w_value,
    w_outgate,
    w_out,
    head_gain,
    second_gain,
    second_gate,
    second_up,
    second_down,
):
    few, block = stream_in.shape
    tp, t, p = lax.axis_size("tp"), lax.axis_index("tp"), lax.axis_index("kvp")
    features = block * lax.axis_size(KV)
    rows = few * tp
    groups = lax.axis_size("kvh")
    tall, across = rows // groups, tp // groups
    wide = block // across
    r, c = lax.div(t, across), lax.rem(t, across)

    half = ret_state.shape[-1] // 2
    decay = jnp.exp(jnp.log1p(-(2.0 ** (-5.0 - t.astype(jnp.float32)))))
    place = lax.div(t * few, tall)
    early = (decay, place, t * few - place * tall)

    first_pair = paired_weights(first_gain, first_gate, first_up)
    second_back = paired_rows(second_down)
    halves = [jnp.concatenate(w, axis=1) for w in ((w_query, w_key), (w_value, w_outgate))]
    halves = jnp.stack(halves).astype(jnp.float32) * mix_gain[:, None]
    downs = first_down.reshape(2, -1, block)
    mix_pair = swapped(jnp.concatenate([downs, halves.astype(jnp.bfloat16)], axis=1))

    cuts = jnp.concatenate(jnp.split(stream_in, across, axis=1), axis=0)
    gathered = spread(cuts, BOTH).reshape(2, tp, tall, wide)
    own = lax.dynamic_slice(gathered, (p, r * across, c * few, 0), (1, across, few, wide)).reshape(tall, wide)
    gathered, own, early = lax.optimization_barrier((gathered, own, early))
    decay, place, offset = early
    back = feed_forward(gathered, first_pair, mix_pair, False)
    own = advance(own, back, 0.5, BOTH)
    held = (own, positions, jnp.arange(half), second_gain)
    own, positions, steps, second_gain = lax.optimization_barrier(held)
    second_pair = paired_weights(second_gain, second_gate, second_up)
    gathered = spread(own, BOTH).reshape(2, tp, tall, wide)
    inverse = 10000.0 ** (-steps.astype(jnp.float32) / half)
    angles = positions.astype(jnp.float32)[:, None] * inverse[None, :]
    cosine, sine = jnp.cos(angles), jnp.sin(angles)
    cosine, sine = jnp.concatenate([cosine, cosine], axis=1), jnp.concatenate([-sine, sine], axis=1)
    gathered, cosine, sine = lax.optimization_barrier((gathered, cosine, sine))
    decay = jnp.broadcast_to(decay, (1, 2 * half))
    ret_out, new_state = retention(gathered, mix_pair, features, head_gain, ret_state, (cosine, sine, decay))
    back = jnp.dot(ret_out, w_out, preferred_element_type=jnp.float32).astype(jnp.bfloat16)
    back = back.reshape(groups, tall, across, wide).transpose(0, 2, 1, 3).reshape(tp, tall, wide)
    own = advance(own, back, 1.0, "tp")
    gathered = spread(own, BOTH).reshape(2, tp, tall, wide)
    own = lax.dynamic_slice(gathered, (p, place * across, offset, 0), (1, across, few, wide))[0]
    own = jnp.concatenate([own[i] for i in range(across)], axis=1)
    gathered, own = lax.optimization_barrier((gathered, own))
    back = feed_forward(gathered, second_pair, second_back, True)
    return advance(own, back, 0.5, BOTH), new_state


def solution(mesh):
    sizes = dict(mesh.shape)
    shape = (sizes["grp"], sizes["kv"] // 2, 2, sizes["tp"])
    fine = Mesh(np.asarray(mesh.devices).reshape(shape), ("grp", *KV, "tp"))
    rows, tall, flat = P(("grp", "tp"), KV), P(KV, "tp"), P("tp", KV)
    in_specs = (
        rows,
        P(("grp", *KV)),
        P(("grp", *KV), "tp", None, None),
        P(KV),
        tall,
        tall,
        flat,
        P(KV),
        tall,
        tall,
        tall,
        tall,
        flat,
        P("tp"),
        P(KV),
        tall,
        tall,
        flat,
    )
    out_specs = (rows, P(("grp", *KV), "tp", None, None))
    return jax.shard_map(per_device, mesh=fine, in_specs=in_specs, out_specs=out_specs, check_vma=False)
```
